32 devices in a mesh: sp: 8 (over z, x), tp: 4 (over y, core).
Axes of the slice: x: 2, y: 2, z: 4, core: 2. Of those that a mesh axis runs over, the one named last changes fastest.
Arguments:
- inputs: bfloat16 [2048, 2048], P('sp', 'tp'), may hold values from -120 to 120
- in_gain: float32 [2048], replicated, may hold values from 0.1 to 1.9
- query_weight: bfloat16 [2048, 1024], P('sp', 'tp'), may hold values from -0.125 to 0.125
- key_weight: bfloat16 [2048, 1024], P('sp', 'tp'), may hold values from -0.125 to 0.125
- value_weight: bfloat16 [2048, 1024], P('sp', 'tp'), may hold values from -0.125 to 0.125
- beta_weight: bfloat16 [2, 2048, 8], replicated, may hold values from -0.125 to 0.125
- decay_weight: bfloat16 [2, 2048, 8], replicated, may hold values from -0.125 to 0.125
- beta_shift: float32 [2, 8], replicated, may hold values from -9 to 1
- decay_pace: float32 [2, 8, 2048], P(None, 'tp', 'sp'), may hold values from 0 to 0.1
- decay_jolt: float32 [2, 8, 2048], P(None, 'tp', 'sp'), may hold values from -1.4 to 0, as said below
- head_gain: float32 [128], replicated, may hold values from 0.1 to 1.9
- glu_value_weight: bfloat16 [2048, 1024], P('sp', 'tp'), may hold values from -0.125 to 0.125
- glu_gate_weight: bfloat16 [2048, 1024], P('sp', 'tp'), may hold values from -0.125 to 0.125
- conv_kernel: bfloat16 [31, 1024], P(None, 'tp'), may hold values from -4 to 4
- conv_gain: float32 [1024], P('tp'), may hold values from 0.1 to 1.9
- out_delta_weight: bfloat16 [1024, 2048], P('tp', 'sp'), may hold values from -0.125 to 0.125
- out_conv_weight: bfloat16 [1024, 2048], P('tp', 'sp'), may hold values from -0.125 to 0.125
Outputs:
- mixed: bfloat16 [2048, 2048], P(('sp', 'tp'))
The draws below stay inside these ranges and needn't reach their ends.
Inputs may be any that keep to these rules, and one draw needn't show every extreme that they name: `decay_jolt`: zero but at a few positions of each direction and head.
All inputs are finite; a program needn't handle non-finite values.
Results may differ from the reference program's by a relative error of at most 0.017.
Values may be sent and summed in bfloat16 or wider, within the bound.
A program may use at most 128 MiB of HBM per device.

```python
import math
import jax
import jax.numpy as jnp
from jax import lax

D = 2048
HEAD = 128
QK_HEADS = 8
V_HEADS = 8
CONV_CH = 1024
KERNEL = 31
BLOCK = 64
T_DEV = 256
SEQ = 2048
N_TP = 4


def slow_flags(key):
    slow_share = 0.5
    return jax.random.uniform(jax.random.fold_in(key, 41), (2, V_HEADS, 1), jnp.float32) < slow_share


def draw_inputs(key, part):
    row_scale = jnp.exp(jax.random.uniform(jax.random.fold_in(key, 2), (SEQ, 1), jnp.float32, 0.0, math.log(10.0)))
    column_scale = jnp.exp(jax.random.uniform(jax.random.fold_in(key, 3), (1, D), jnp.float32, 0.0, math.log(3.0)))
    base_draw = jnp.clip(jax.random.normal(jax.random.fold_in(key, 1), (SEQ, D), jnp.float32), -4.0, 4.0)
    return (base_draw * row_scale * column_scale).astype(jnp.bfloat16)


def draw_beta_shift(key, part):
    slow_heads = slow_flags(key)[:, :, 0]
    fast_shift = jax.random.uniform(jax.random.fold_in(key, 42), (2, V_HEADS), jnp.float32, -1.0, 1.0)
    strength = jnp.exp(jax.random.uniform(jax.random.fold_in(key, 46), (2, V_HEADS), jnp.float32, math.log(0.2), math.log(0.5)))
    slow_shift = jnp.log(strength * HEAD / SEQ)
    return jnp.where(slow_heads, slow_shift, fast_shift)


def draw_decay_pace(key, part):
    slow_heads = slow_flags(key)
    fast_rate = jnp.exp(jax.random.uniform(jax.random.fold_in(key, 43), (2, V_HEADS, 1), jnp.float32, math.log(0.015), math.log(0.05)))
    slow_rate = jnp.exp(jax.random.uniform(jax.random.fold_in(key, 44), (2, V_HEADS, 1), jnp.float32, math.log(0.2), math.log(0.6))) / SEQ
    factor = jnp.exp(jax.random.uniform(jax.random.fold_in(key, 45), (2, V_HEADS, SEQ // T_DEV, 1), jnp.float32, math.log(0.5), math.log(2.0)))
    factor = jnp.broadcast_to(factor, (2, V_HEADS, SEQ // T_DEV, T_DEV)).reshape(2, V_HEADS, SEQ)
    return jnp.where(slow_heads, slow_rate, fast_rate) * factor


def draw_decay_jolt(key, part):
    places = jax.random.randint(jax.random.fold_in(key, 51), (2, V_HEADS, 2, 1), 0, SEQ)
    depth = jnp.log(jax.random.uniform(jax.random.fold_in(key, 52), (2, V_HEADS, 2, 1), jnp.float32, 0.5, 0.8))
    position = jnp.arange(SEQ, dtype=jnp.int32)
    return jnp.sum(jnp.where(position[None, None, None, :] == places, depth, 0.0), axis=2)


def draw_conv_kernel(key, part):
    channel = jnp.arange(CONV_CH, dtype=jnp.float32) / max(CONV_CH - 1, 1)
    rise_factor = 3.0
    scale = jnp.exp(math.log(rise_factor) * channel) * (0.6 / math.sqrt(KERNEL))
    base_draw = jnp.clip(jax.random.normal(jax.random.fold_in(key, 62), (KERNEL, CONV_CH), jnp.float32), -4.0, 4.0)
    return (base_draw * scale[None, :]).astype(jnp.bfloat16)


def block_levels(own_key, dims, split, low, top_value):
    factor_of, own = 1.0, jax.random.fold_in(own_key, 6)
    for dim, shards_of in split:
        heights = jnp.exp(jax.random.uniform(jax.random.fold_in(own, dim), (shards_of,), jnp.float32, low / len(split), top_value / len(split)))
        factor_of = factor_of * jnp.repeat(heights, dims[dim] // shards_of).reshape([-1 if axis == dim else 1 for axis in range(len(dims))])
    return factor_of


def noise(key, dims, width, most, shards=(), kind=jnp.bfloat16):
    level = block_levels(key, dims, shards, -0.22, 0.18) if shards else 1.0
    entries = jax.random.normal(key, dims, jnp.float32) * width * level
    return jnp.minimum(jnp.maximum(entries, -most), most).astype(kind)


def setup_inputs(seed: int = 0) -> dict:
    streams_of = jax.random.split(jax.random.key(seed), 18)
    inputs = draw_inputs(jax.random.fold_in(streams_of[17], 71), 0)
    in_gain = jnp.clip(1.0 + 0.18 * jax.random.normal(streams_of[1], (D,), jnp.float32), 0.1, 1.9)
    query_weight = noise(streams_of[2], (D, QK_HEADS * HEAD), D ** -0.5, 0.125, ((0, 8), (1, 4)))
    key_weight = noise(streams_of[3], (D, QK_HEADS * HEAD), D ** -0.5, 0.125, ((0, 8), (1, 4)))
    value_weight = noise(streams_of[4], (D, V_HEADS * HEAD), D ** -0.5, 0.125, ((0, 8), (1, 4)))
    beta_weight = noise(streams_of[5], (2, D, V_HEADS), D ** -0.5, 0.125)
    decay_weight = noise(streams_of[6], (2, D, V_HEADS), D ** -0.5, 0.125)
    beta_shift = draw_beta_shift(jax.random.fold_in(streams_of[17], 71), 0)
    decay_pace = draw_decay_pace(jax.random.fold_in(streams_of[17], 71), 0)
    decay_jolt = draw_decay_jolt(jax.random.fold_in(streams_of[17], 71), 0)
    head_gain = jnp.clip(1.0 + 0.18 * jax.random.normal(streams_of[10], (HEAD,), jnp.float32), 0.1, 1.9)
    glu_value_weight = noise(streams_of[11], (D, CONV_CH), D ** -0.5, 0.125, ((0, 8), (1, 4)))
    glu_gate_weight = noise(streams_of[12], (D, CONV_CH), D ** -0.5, 0.125, ((0, 8), (1, 4)))
    conv_kernel = draw_conv_kernel(jax.random.fold_in(streams_of[17], 71), 0)
    conv_gain = jnp.clip(1.0 + 0.18 * jax.random.normal(streams_of[14], (CONV_CH,), jnp.float32), 0.1, 1.9)
    out_delta_weight = noise(streams_of[15], (V_HEADS * HEAD, D), (V_HEADS * HEAD + CONV_CH) ** -0.5, 0.125, ((0, 4), (1, 8)))
    out_conv_weight = noise(streams_of[16], (CONV_CH, D), (V_HEADS * HEAD + CONV_CH) ** -0.5, 0.125, ((0, 4), (1, 8)))
    return {"inputs": inputs, "in_gain": in_gain, "query_weight": query_weight, "key_weight": key_weight, "value_weight": value_weight, "beta_weight": beta_weight, "decay_weight": decay_weight, "beta_shift": beta_shift, "decay_pace": decay_pace, "decay_jolt": decay_jolt, "head_gain": head_gain, "glu_value_weight": glu_value_weight, "glu_gate_weight": glu_gate_weight, "conv_kernel": conv_kernel, "conv_gain": conv_gain, "out_delta_weight": out_delta_weight, "out_conv_weight": out_conv_weight}


highest = lax.Precision.HIGHEST

def matmul_high(left_side, right_side):
    return jnp.matmul(left_side, right_side, precision=highest)

def unit_lower_inverse(matrix):
    order_size = matrix.shape[-1]
    leading = matrix.shape[:-2]
    inverse = jnp.ones(leading + (order_size, 1, 1), jnp.float32)
    size_now = 1
    while size_now < order_size:
        pair_count = order_size // (2 * size_now)
        halves = inverse.reshape(leading + (pair_count, 2, size_now, size_now))
        upper_inv = halves[..., 0, :, :]
        lower_inv = halves[..., 1, :, :]
        block_grid = matrix.reshape(leading + (pair_count, 2 * size_now, pair_count, 2 * size_now))
        diagonal = jnp.moveaxis(jnp.diagonal(block_grid, axis1=-4, axis2=-2), -1, -3)
        corner = diagonal[..., size_now:, :size_now]
        below = -matmul_high(lower_inv, matmul_high(corner, upper_inv))
        top_half = jnp.concatenate([upper_inv, jnp.zeros_like(below)], axis=-1)
        bottom_half = jnp.concatenate([below, lower_inv], axis=-1)
        inverse = jnp.concatenate([top_half, bottom_half], axis=-2)
        size_now = 2 * size_now
    return inverse.reshape(leading + (order_size, order_size))

def block_terms(queries, key_rows, values, beta_gate, log_decay):
    span = key_rows.shape[-2]
    cumulative = jnp.cumsum(log_decay, axis=-1)
    lower_mask = jnp.tril(jnp.ones((span, span), dtype=bool))
    strict = jnp.tril(jnp.ones((span, span), dtype=bool), -1)
    log_gap = cumulative[..., :, None] - cumulative[..., None, :]
    decay_mask = jnp.where(lower_mask, jnp.exp(jnp.where(lower_mask, log_gap, 0.0)), 0.0)
    key_inner = matmul_high(key_rows, jnp.swapaxes(key_rows, -1, -2))
    below_part = jnp.where(strict, beta_gate[..., :, None] * key_inner * decay_mask, 0.0)
    inverse = unit_lower_inverse(below_part + jnp.eye(span, dtype=jnp.float32))
    fresh = matmul_high(inverse, values * beta_gate[..., None])
    weighted = matmul_high(inverse, key_rows * (beta_gate * jnp.exp(cumulative))[..., None])
    scores = matmul_high(queries, jnp.swapaxes(key_rows, -1, -2)) * decay_mask
    readout = queries * jnp.exp(cumulative)[..., None] - matmul_high(scores, weighted)
    tail_keys = jnp.swapaxes(key_rows * jnp.exp(cumulative[..., -1:] - cumulative)[..., None], -1, -2)
    identity = jnp.eye(key_rows.shape[-1], dtype=jnp.float32)
    carry_map = jnp.exp(cumulative[..., -1])[..., None, None] * identity - matmul_high(tail_keys, weighted)
    carry_add = matmul_high(tail_keys, fresh)
    within = matmul_high(scores, fresh)
    return (carry_map, carry_add, readout, within)

def layer_norm_rows(inputs, gain):
    as_float = inputs.astype(jnp.float32)
    mean_row = lax.optimization_barrier(jnp.mean(as_float, axis=-1, keepdims=True))
    spread = lax.optimization_barrier(jnp.mean(jnp.square(as_float - mean_row), axis=-1, keepdims=True))
    return ((as_float - mean_row) * lax.rsqrt(spread + 1e-05) * gain).astype(jnp.bfloat16)

def to_blocks(tensor):
    return tensor.reshape((tensor.shape[0] // BLOCK, BLOCK) + tensor.shape[1:])

def one_direction(queries, key_rows, values, beta_gate, log_decay):
    carry_map, carry_add, readout, within = block_terms(to_blocks(queries), to_blocks(key_rows), to_blocks(values), to_blocks(beta_gate), to_blocks(log_decay))

    def advance(carried, block_parts):
        step_map, step_add, step_read, step_within = block_parts
        return (matmul_high(step_map, carried) + step_add, matmul_high(step_read, carried) + step_within)
    initial = jnp.zeros((queries.shape[1], values.shape[1]), jnp.float32)
    _, outputs = lax.scan(advance, initial, (carry_map, carry_add, readout, within))
    return outputs.reshape(values.shape)

def reference(inputs, in_gain, query_weight, key_weight, value_weight, beta_weight, decay_weight, beta_shift, decay_pace, decay_jolt, head_gain, glu_value_weight, glu_gate_weight, conv_kernel, conv_gain, out_delta_weight, out_conv_weight):
    normed = layer_norm_rows(inputs, in_gain)
    queries = jnp.dot(normed, query_weight, preferred_element_type=jnp.float32).astype(jnp.bfloat16)
    key_proj = jnp.dot(normed, key_weight, preferred_element_type=jnp.float32).astype(jnp.bfloat16)
    value_proj = jnp.dot(normed, value_weight, preferred_element_type=jnp.float32).astype(jnp.bfloat16)
    glu_value = jnp.dot(normed, glu_value_weight, preferred_element_type=jnp.float32).astype(jnp.bfloat16)
    glu_gate = jnp.dot(normed, glu_gate_weight, preferred_element_type=jnp.float32).astype(jnp.bfloat16)
    beta_cols = jnp.moveaxis(beta_weight, 0, 1).reshape(D, 2 * V_HEADS)
    decay_cols = jnp.moveaxis(decay_weight, 0, 1).reshape(D, 2 * V_HEADS)
    beta_pre = jnp.transpose(jnp.dot(normed, beta_cols, preferred_element_type=jnp.float32).reshape(SEQ, 2, V_HEADS), (1, 2, 0))
    decay_pre = jnp.transpose(jnp.dot(normed, decay_cols, preferred_element_type=jnp.float32).reshape(SEQ, 2, V_HEADS), (1, 2, 0))
    beta_gate = jax.nn.sigmoid(beta_pre + beta_shift[:, :, None])
    log_decay = -decay_pace * jax.nn.softplus(decay_pre) + decay_jolt
    group_size = V_HEADS // QK_HEADS

    def head_output(head_index):
        key_start = head_index // group_size * HEAD
        q_head = jax.nn.silu(lax.dynamic_slice_in_dim(queries, key_start, HEAD, 1).astype(jnp.float32))
        k_head = jax.nn.silu(lax.dynamic_slice_in_dim(key_proj, key_start, HEAD, 1).astype(jnp.float32))
        k_head = k_head * lax.rsqrt(lax.optimization_barrier(jnp.sum(jnp.square(k_head), axis=-1, keepdims=True)) + 1e-06)
        v_head = lax.dynamic_slice_in_dim(value_proj, head_index * HEAD, HEAD, 1).astype(jnp.float32)
        gates = beta_gate[:, head_index]
        decays = log_decay[:, head_index]
        forward = one_direction(q_head, k_head, v_head, gates[0], decays[0])
        backward = jnp.flip(one_direction(jnp.flip(q_head, 0), jnp.flip(k_head, 0), jnp.flip(v_head, 0), jnp.flip(gates[1], 0), jnp.flip(decays[1], 0)), 0)
        combined = forward + backward
        scaled = combined * lax.rsqrt(lax.optimization_barrier(jnp.mean(jnp.square(combined), axis=-1, keepdims=True)) + 1e-06) * head_gain
        return scaled.astype(jnp.bfloat16)
    delta_heads = lax.map(head_output, jnp.arange(V_HEADS, dtype=jnp.int32))
    delta_out = jnp.transpose(delta_heads, (1, 0, 2)).reshape(SEQ, V_HEADS * HEAD)
    gated = (glu_value.astype(jnp.float32) * jax.nn.sigmoid(glu_gate.astype(jnp.float32))).astype(jnp.bfloat16)
    half_width = KERNEL // 2
    padded = jnp.pad(gated, ((half_width, half_width), (0, 0)))
    filtered = jnp.zeros((SEQ, CONV_CH), jnp.float32)
    for tap_index in range(KERNEL):
        filtered = filtered + padded[tap_index:tap_index + SEQ].astype(jnp.float32) * conv_kernel[tap_index].astype(jnp.float32)
    mean_row = lax.optimization_barrier(jnp.mean(filtered, axis=-1, keepdims=True))
    second = lax.optimization_barrier(jnp.mean(filtered * filtered, axis=-1, keepdims=True))
    conv_out = jax.nn.silu((filtered - mean_row) * lax.rsqrt(second - mean_row * mean_row + 1e-05) * conv_gain).astype(jnp.bfloat16)
    delta_group = V_HEADS * HEAD // N_TP
    conv_group = CONV_CH // N_TP
    totals = jnp.zeros((SEQ, D), jnp.float32)
    for group_index in range(N_TP):
        d_lo = group_index * delta_group
        c_lo = group_index * conv_group
        partial_value = jnp.dot(delta_out[:, d_lo:d_lo + delta_group], out_delta_weight[d_lo:d_lo + delta_group], preferred_element_type=jnp.float32)
        partial_value = partial_value + jnp.dot(conv_out[:, c_lo:c_lo + conv_group], out_conv_weight[c_lo:c_lo + conv_group], preferred_element_type=jnp.float32)
        totals = totals + partial_value.astype(jnp.bfloat16).astype(jnp.float32)
    return totals.astype(jnp.bfloat16)
```

```python
import functools

import jax
import jax.numpy as jnp
from jax import lax
from jax.experimental import pallas as pl
from jax.experimental.pallas import tpu as pltpu
from jax.sharding import PartitionSpec as P

HEAD = 128
QK_HEADS = 8
V_HEADS = 8
CONV_CH = 1024
KERNEL = 31
BLOCK = 64


highest = lax.Precision.HIGHEST


def prefix_2(shard, axis, combine, identity, reverse):
    peers, position = (lax.axis_size(axis), lax.axis_index(axis))
    everything = jax.tree.map(
        lambda part, kind: lax.all_gather(part.astype(kind), axis),
        shard,
        (jnp.bfloat16, jnp.bfloat16),
    )
    start = jax.tree.map(
        lambda part, zero: jnp.broadcast_to(jnp.asarray(zero, part.dtype), part.shape),
        shard,
        identity,
    )

    def lap(k, before):
        at = peers - 1 - k if reverse else k
        reached = at > position if reverse else at < position
        new = combine(
            before, jax.tree.map(lambda part, own: part[at].astype(own.dtype), everything, shard)
        )
        return jax.tree.map(lambda a, b: jnp.where(reached, a, b), new, before)

    return lax.fori_loop(0, peers, lap, start)


def padded_2(cells, sides, width):
    for axis, dim in sides:
        count = lax.axis_size(axis)
        ends = count - 1
        head = lax.slice_in_dim(cells, 0, width, axis=dim)
        tail = lax.slice_in_dim(cells, cells.shape[dim] - width, cells.shape[dim], axis=dim)
        cells = jnp.concatenate(
            [
                lax.ppermute(tail, axis, [(i, (i + 1) % count) for i in range(ends)]),
                cells,
                lax.ppermute(head, axis, [((i + 1) % count, i) for i in range(ends)]),
            ],
            axis=dim,
        )
    return cells


def matmul_high(left_side, right_side):
    return jnp.matmul(left_side, right_side, precision=highest)


def unit_lower_inverse(matrix):
    order_size = matrix.shape[-1]
    leading = matrix.shape[:-2]
    inverse = jnp.ones(leading + (order_size, 1, 1), jnp.float32)
    size_now = 1
    while size_now < order_size:
        pair_count = order_size // (2 * size_now)
        halves = inverse.reshape(leading + (pair_count, 2, size_now, size_now))
        upper_inv = halves[..., 0, :, :]
        lower_inv = halves[..., 1, :, :]
        block_grid = matrix.reshape(leading + (pair_count, 2 * size_now, pair_count, 2 * size_now))
        diagonal = jnp.moveaxis(jnp.diagonal(block_grid, axis1=-4, axis2=-2), -1, -3)
        corner = diagonal[..., size_now:, :size_now]
        below = -matmul_high(lower_inv, matmul_high(corner, upper_inv))
        top_half = jnp.concatenate([upper_inv, jnp.zeros_like(below)], axis=-1)
        bottom_half = jnp.concatenate([below, lower_inv], axis=-1)
        inverse = jnp.concatenate([top_half, bottom_half], axis=-2)
        size_now = 2 * size_now
    return inverse.reshape(leading + (order_size, order_size))


def block_terms(queries, key_rows, values, beta_gate, log_decay):
    span = key_rows.shape[-2]
    cumulative = jnp.cumsum(log_decay, axis=-1)
    lower_mask = jnp.tril(jnp.ones((span, span), dtype=bool))
    strict = jnp.tril(jnp.ones((span, span), dtype=bool), -1)
    log_gap = cumulative[..., :, None] - cumulative[..., None, :]
    decay_mask = jnp.where(lower_mask, jnp.exp(jnp.where(lower_mask, log_gap, 0.0)), 0.0)
    key_inner = matmul_high(key_rows, jnp.swapaxes(key_rows, -1, -2))
    below_part = jnp.where(strict, beta_gate[..., :, None] * key_inner * decay_mask, 0.0)
    inverse = unit_lower_inverse(below_part + jnp.eye(span, dtype=jnp.float32))
    fresh = matmul_high(inverse, values * beta_gate[..., None])
    weighted = matmul_high(inverse, key_rows * (beta_gate * jnp.exp(cumulative))[..., None])
    scores = matmul_high(queries, jnp.swapaxes(key_rows, -1, -2)) * decay_mask
    readout = queries * jnp.exp(cumulative)[..., None] - matmul_high(scores, weighted)
    tail_keys = jnp.swapaxes(
        key_rows * jnp.exp(cumulative[..., -1:] - cumulative)[..., None], -1, -2
    )
    identity = jnp.eye(key_rows.shape[-1], dtype=jnp.float32)
    carry_map = jnp.exp(cumulative[..., -1])[..., None, None] * identity - matmul_high(
        tail_keys, weighted
    )
    carry_add = matmul_high(tail_keys, fresh)
    within = matmul_high(scores, fresh)
    return (carry_map, carry_add, readout, within)


def layer_norm_rows(inputs, gain):
    as_float = inputs.astype(jnp.float32)
    mean_row = jnp.mean(as_float, axis=-1, keepdims=True)
    spread = jnp.mean(jnp.square(as_float - mean_row), axis=-1, keepdims=True)
    return ((as_float - mean_row) * lax.rsqrt(spread + 1e-05) * gain).astype(jnp.bfloat16)


def compose(earlier, later):
    return (matmul_high(later[0], earlier[0]), matmul_high(later[0], earlier[1]) + later[1])


def local_maps(queries, key_rows, values, beta_gate, log_decay):
    head_count, length_dev, key_width = queries.shape
    value_width = values.shape[-1]
    block_count = length_dev // BLOCK

    def split_blocks(tensor):
        return tensor.reshape((head_count, block_count, BLOCK) + tensor.shape[2:])

    carry_map, carry_add, readout, within = block_terms(
        split_blocks(queries),
        split_blocks(key_rows),
        split_blocks(values),
        split_blocks(beta_gate),
        split_blocks(log_decay),
    )
    identity = jnp.broadcast_to(
        jnp.eye(key_width, dtype=jnp.float32), (head_count, key_width, key_width)
    )
    nothing = jnp.zeros((head_count, key_width, value_width), jnp.float32)

    def advance(prefix, block_parts):
        prefix_map, prefix_add = prefix
        step_map, step_add, step_read = block_parts
        reach_now = matmul_high(step_read, prefix_map)
        offset_now = matmul_high(step_read, prefix_add)
        return (
            (matmul_high(step_map, prefix_map), matmul_high(step_map, prefix_add) + step_add),
            (reach_now, offset_now),
        )

    moved = (
        jnp.moveaxis(carry_map, 1, 0),
        jnp.moveaxis(carry_add, 1, 0),
        jnp.moveaxis(readout, 1, 0),
    )
    totals, (reach_map, offset) = lax.scan(advance, (identity, nothing), moved)
    reach_map = jnp.moveaxis(reach_map, 0, 1).reshape(head_count, length_dev, key_width)
    offset = (jnp.moveaxis(offset, 0, 1) + within).reshape(head_count, length_dev, value_width)
    return (totals, reach_map, offset)


def on_device(
    inputs,
    in_gain,
    query_weight,
    key_weight,
    value_weight,
    beta_weight,
    decay_weight,
    beta_shift,
    decay_pace,
    decay_jolt,
    head_gain,
    glu_value_weight,
    glu_gate_weight,
    conv_kernel,
    conv_gain,
    out_delta_weight,
    out_conv_weight,
):
    gathered = lax.all_gather(inputs, "tp", axis=1, tiled=True)
    normed = layer_norm_rows(gathered, in_gain)
    row_count = normed.shape[0]

    def add_rows(shard_rows):
        return jnp.dot(normed, shard_rows, preferred_element_type=jnp.float32)

    shards = (
        lax.all_gather(query_weight, "sp", axis=0, tiled=True),
        lax.all_gather(key_weight, "sp", axis=0, tiled=True),
        lax.all_gather(value_weight, "sp", axis=0, tiled=True),
        lax.all_gather(glu_value_weight, "sp", axis=0, tiled=True),
        lax.all_gather(glu_gate_weight, "sp", axis=0, tiled=True),
    )
    projected = tuple((add_rows(shard_rows) for shard_rows in shards))
    delta_sums = projected[:3]
    conv_sums = projected[3:]
    queries, key_proj, value_proj = (summed.astype(jnp.bfloat16) for summed in delta_sums)
    local_heads = value_proj.shape[1] // HEAD
    group_size = V_HEADS // QK_HEADS
    head_first = lax.axis_index("tp") * local_heads

    def by_head(matrix, head_total):
        return jnp.transpose(
            matrix.astype(jnp.float32).reshape(row_count, head_total, HEAD), (1, 0, 2)
        )

    query_heads = jnp.repeat(
        jax.nn.silu(by_head(queries, local_heads // group_size)), group_size, axis=0
    )
    key_heads = jax.nn.silu(by_head(key_proj, local_heads // group_size))
    key_heads = key_heads * lax.rsqrt(
        jnp.sum(jnp.square(key_heads), axis=-1, keepdims=True) + 1e-06
    )
    key_heads = jnp.repeat(key_heads, group_size, axis=0)
    value_heads = by_head(value_proj, local_heads)
    own_beta = lax.dynamic_slice_in_dim(beta_weight, head_first, local_heads, 2)
    own_decay = lax.dynamic_slice_in_dim(decay_weight, head_first, local_heads, 2)
    beta_pre = jnp.einsum("td,edh->eht", normed, own_beta, preferred_element_type=jnp.float32)
    decay_pre = jnp.einsum("td,edh->eht", normed, own_decay, preferred_element_type=jnp.float32)
    own_shift = lax.dynamic_slice_in_dim(beta_shift, head_first, local_heads, 1)
    beta_gate = jax.nn.sigmoid(beta_pre + own_shift[:, :, None])
    log_decay = -decay_pace * jax.nn.softplus(decay_pre) + decay_jolt
    identity = jnp.broadcast_to(jnp.eye(HEAD, dtype=jnp.float32), (local_heads, HEAD, HEAD))
    nothing = jnp.zeros((local_heads, HEAD, HEAD), jnp.float32)
    forward_maps, forward_reach, forward_offset = local_maps(
        query_heads, key_heads, value_heads, beta_gate[0], log_decay[0]
    )
    entry_forward = prefix_2(
        (forward_maps[0], forward_maps[1]), "sp", compose, (identity, nothing), False
    )
    forward_out = matmul_high(forward_reach, entry_forward[1]) + forward_offset
    backward_maps, backward_reach, backward_offset = local_maps(
        jnp.flip(query_heads, 1),
        jnp.flip(key_heads, 1),
        jnp.flip(value_heads, 1),
        jnp.flip(beta_gate[1], 1),
        jnp.flip(log_decay[1], 1),
    )
    entry_backward = prefix_2(
        (backward_maps[0], backward_maps[1]), "sp", compose, (identity, nothing), True
    )
    backward_out = jnp.flip(matmul_high(backward_reach, entry_backward[1]) + backward_offset, 1)
    combined = forward_out + backward_out
    scaled = (
        combined
        * lax.rsqrt(jnp.mean(jnp.square(combined), axis=-1, keepdims=True) + 1e-06)
        * head_gain
    )
    delta_out = (
        jnp.transpose(scaled, (1, 0, 2)).reshape(row_count, local_heads * HEAD).astype(jnp.bfloat16)
    )
    glu_value, glu_gate = (summed.astype(jnp.bfloat16) for summed in conv_sums)
    gated = (glu_value.astype(jnp.float32) * jax.nn.sigmoid(glu_gate.astype(jnp.float32))).astype(
        jnp.bfloat16
    )
    padded = padded_2(gated, (("sp", 0),), KERNEL // 2)
    filtered = jnp.zeros(gated.shape, jnp.float32)
    for tap_index in range(KERNEL):
        filtered = filtered + padded[tap_index : tap_index + row_count].astype(
            jnp.float32
        ) * conv_kernel[tap_index].astype(jnp.float32)
    totals = lax.psum((jnp.sum(filtered, axis=1), jnp.sum(filtered * filtered, axis=1)), "tp")
    mean_row = totals[0][:, None] / CONV_CH
    second = totals[1][:, None] / CONV_CH
    conv_out = jax.nn.silu(
        (filtered - mean_row) * lax.rsqrt(second - mean_row * mean_row + 1e-05) * conv_gain
    ).astype(jnp.bfloat16)
    delta_whole, conv_whole = (
        lax.all_gather(out_delta_weight, "sp", axis=1, tiled=True),
        lax.all_gather(out_conv_weight, "sp", axis=1, tiled=True),
    )
    delta_part = jnp.dot(delta_out, delta_whole, preferred_element_type=jnp.float32)
    conv_part = jnp.dot(conv_out, conv_whole, preferred_element_type=jnp.float32)
    return lax.psum_scatter(
        (delta_part + conv_part).astype(jnp.bfloat16), "tp", scatter_dimension=0, tiled=True
    )


MESH = pl.DeviceIdType.MESH
F32 = jnp.float32
BF16 = jnp.bfloat16
VM = pl.BlockSpec(memory_space=pltpu.VMEM)


def greet(peers):
    barrier = pltpu.get_barrier_semaphore()
    for peer in peers:
        pl.semaphore_signal(barrier, inc=1, device_id=peer, device_id_type=MESH)
    pl.semaphore_wait(barrier, len(peers))


def ring_peers(n):
    s, t = lax.axis_index("sp"), lax.axis_index("tp")
    half = n // 2
    z, x = s // 2, s % 2
    partner = (z * 2 + (1 - x), t)
    stride = [(((z + d) % half) * 2 + x, t) for d in range(1, half)]
    return s, t, z, x, half, partner, stride


def rcopy(src, dst, send, recv, peer):
    return pltpu.make_async_remote_copy(
        src_ref=src, dst_ref=dst, send_sem=send, recv_sem=recv, device_id=peer, device_id_type=MESH
    )


def dot(a, b):
    return jnp.dot(a, b, preferred_element_type=F32)


def project_kernel(n, nt, n_in, *refs):
    x_ref, gain_ref, wg_ref = refs[:3]
    w_refs = refs[3 : 3 + n_in]
    qkv_ref, gated_ref, pre_ref = refs[3 + n_in : 6 + n_in]
    xbuf, normed, acc, wz, wx, xs, xr, zs, zr, ps, pr = refs[6 + n_in :]
    s, t, z, x, half, partner, stride = ring_peers(n)
    others = [(s, (t + d) % nt) for d in range(1, nt)]
    greet(others + [partner] + stride)
    order = [d for d in range(half - 1)]
    x_copies = [rcopy(x_ref, xbuf.at[d], xs.at[d], xr.at[d], others[d]) for d in range(nt - 1)]
    for c in x_copies:
        c.start()
    own_x = [rcopy(w_refs[w], wx.at[0, w], ps.at[0, w], pr.at[0, w], partner) for w in range(n_in)]
    own_z = [
        [rcopy(w_refs[w], wz.at[d, w], zs.at[d, w], zr.at[d, w], stride[d]) for d in order]
        for w in range(n_in)
    ]
    for w in range(n_in):
        for d in order:
            own_z[w][d].start()
        own_x[w].start()
    for c in x_copies:
        c.wait_recv()
    rows, part = x_ref.shape
    block = w_refs[0].shape[0]
    per = part // block
    total = rows * 0 + part * nt
    chunks = [(t, x_ref)] + [((t + nt - 1 - d) % nt, xbuf.at[d]) for d in range(nt - 1)]
    mean = sum(jnp.sum(r[...].astype(F32), axis=1, keepdims=True) for _, r in chunks) / total
    var = (
        sum(jnp.sum(jnp.square(r[...].astype(F32) - mean), axis=1, keepdims=True) for _, r in chunks)
        / total
    )
    inv = lax.rsqrt(var + 1e-05)
    for src, r in chunks:
        y = (r[...].astype(F32) - mean) * inv
        for p in range(per):
            b = src * per + p
            g = gain_ref[pl.ds(b, 1), :]
            normed[b] = (y[:, p * block : (p + 1) * block] * g).astype(BF16)
    pre = dot(normed[0], wg_ref[0:block, :])
    for b in range(1, n):
        pre = pre + dot(normed[b], wg_ref[b * block : (b + 1) * block, :])
    pre_ref[...] = pre
    width = w_refs[0].shape[1]
    forwards = []
    for w in range(n_in):
        value = dot(normed[s], w_refs[w][...])
        for d in order:
            own_z[w][d].wait_recv()
            f = rcopy(wz.at[d, w], wx.at[d + 1, w], ps.at[d + 1, w], pr.at[d + 1, w], partner)
            f.start()
            forwards.append(f)
            src = ((z + half - 1 - d) % half) * 2 + x
            value = value + dot(normed[src], wz[d, w])
        acc[:, w * width : (w + 1) * width] = value
    for w in range(n_in):
        own_x[w].wait_recv()
        value = acc[:, w * width : (w + 1) * width]
        value = value + dot(normed[z * 2 + (1 - x)], wx[0, w])
        for d in order:
            forwards[w * len(order) + d].wait_recv()
            src = ((z + half - 1 - d) % half) * 2 + (1 - x)
            value = value + dot(normed[src], wx[d + 1, w])
        acc[:, w * width : (w + 1) * width] = value
    qkv_ref[...] = acc[:, : 3 * width].astype(BF16)
    glu_value = acc[:, 3 * width : 4 * width].astype(BF16).astype(F32)
    glu_gate = acc[:, 4 * width : 5 * width].astype(BF16).astype(F32)
    gated_ref[...] = (glu_value * jax.nn.sigmoid(glu_gate)).astype(BF16)
    for c in x_copies + own_x + forwards + [c for row in own_z for c in row]:
        c.wait_send()


def dot3(a, b):
    ah, bh = a.astype(BF16), b.astype(BF16)
    al, bl = (a - ah.astype(F32)).astype(BF16), (b - bh.astype(F32)).astype(BF16)
    return dot(ah, bh) + (dot(ah, bl) + dot(al, bh))


def delta_kernel(heads, qkv_ref, pre_ref, shift_ref, pace_ref, jolt_ref, ma_ref, read_ref, within_ref):
    span = qkv_ref.shape[0]
    width = heads * HEAD
    rows = jnp.transpose(pre_ref[...])
    beta = jax.nn.sigmoid(rows[0:8] + shift_ref[...])
    log_decay = -pace_ref[...] * jax.nn.softplus(rows[8:16]) + jolt_ref[...]
    i = lax.broadcasted_iota(jnp.int32, (span, span), 0)
    j = lax.broadcasted_iota(jnp.int32, (span, span), 1)
    high = lax.Precision.HIGHEST
    upto = jnp.dot(log_decay, (i <= j).astype(F32), precision=high, preferred_element_type=F32)
    onto = jnp.dot(log_decay, (i >= j).astype(F32), precision=high, preferred_element_type=F32)
    which = lax.broadcasted_iota(jnp.int32, (8, span), 0)
    cum = jnp.where(which < heads, upto, onto)
    cols = jnp.transpose(
        jnp.concatenate([beta, cum, jnp.zeros((128 - 16, span), F32)], axis=0)
    )
    eye = (i == j).astype(F32)
    eye_head = (
        lax.broadcasted_iota(jnp.int32, (HEAD, HEAD), 0)
        == lax.broadcasted_iota(jnp.int32, (HEAD, HEAD), 1)
    ).astype(F32)
    level = i ^ j
    for h in range(heads):
        lo = h * HEAD
        q = jax.nn.silu(qkv_ref[:, lo : lo + HEAD].astype(F32))
        k = jax.nn.silu(qkv_ref[:, width + lo : width + lo + HEAD].astype(F32))
        k = k * lax.rsqrt(jnp.sum(jnp.square(k), axis=1, keepdims=True) + 1e-06)
        v = qkv_ref[:, 2 * width + lo : 2 * width + lo + HEAD].astype(F32)
        kt = jnp.transpose(k)
        kk = dot3(k, kt)
        qk = dot(q.astype(BF16), kt.astype(BF16))
        total = jnp.zeros((span, HEAD), F32)
        for e in range(2):
            c = e * heads + h
            beta_col = cols[:, c : c + 1]
            cum_col = cols[:, 8 + c : 9 + c]
            cum_row = cum[c : c + 1, :]
            keep = (i >= j) if e == 0 else (i <= j)
            gap = jnp.exp(jnp.where(keep, cum_col - cum_row, 0.0))
            decay = jnp.where(keep, gap, 0.0)
            below = jnp.where(i == j, 0.0, beta_col * kk * decay)
            inverse = eye - jnp.where(level < 2, below, 0.0)
            size = 2
            while size < span:
                corner = jnp.where((level >= size) & (level < 2 * size), below, 0.0)
                inverse = inverse - dot3(inverse, dot3(corner, inverse))
                size = 2 * size
            grown = jnp.exp(cum_col)
            rhs = jnp.concatenate([v * beta_col, k * (beta_col * grown)], axis=1)
            solved = dot3(inverse, rhs)
            solved_b = solved.astype(BF16)
            out = dot((qk * decay).astype(BF16), solved_b)
            total = total + out[:, :HEAD]
            read_ref[c] = (q * grown - out[:, HEAD:]).astype(BF16)
            end = cum[c : c + 1, span - 1 : span] if e == 0 else cum[c : c + 1, 0:1]
            tail = jnp.transpose(k * jnp.exp(end - cum_col))
            state = dot3(tail, solved)
            ma_ref[c, :, :HEAD] = (jnp.exp(end) * eye_head - state[:, HEAD:]).astype(BF16)
            ma_ref[c, :, HEAD:] = state[:, :HEAD].astype(BF16)
        within_ref[h] = total


def finish_kernel(
    n, nt, heads, channels,
    ma_ref, read_ref, within_ref, gated_ref, taps_ref, cgain_ref, hgain_ref, ow_ref,
    out_ref,
    near, pair, far, halo, conv_pad, stat, stats, wz, wx, part, parts,
    ns, nr, fs, fr, hs, hr, ss, sr, zs, zr, ps, pr, rs, rr,
):
    s, t, z, x, half, partner, stride = ring_peers(n)
    others = [(s, (t + d) % nt) for d in range(1, nt)]
    greet(others + [((s + d) % n, t) for d in range(1, n)])
    rows, width = gated_ref.shape
    edge = 16

    def at(offset):
        return ((s + offset + n) % n, t)

    def inside(offset):
        return (s < n - offset) if offset > 0 else (s >= -offset)

    steps = []
    for d in (1, 2):
        for e in range(2):
            go = d if e == 0 else -d
            lo = e * heads
            steps.append((go, rcopy(ma_ref.at[pl.ds(lo, heads)], near.at[e, d - 1], ns.at[e, d - 1], nr.at[e, d - 1], at(go)), near.at[e, d - 1]))
    sides = [
        (1, rcopy(gated_ref.at[pl.ds(rows - edge, edge)], halo.at[0], hs.at[0], hr.at[0], at(1)), halo.at[0]),
        (-1, rcopy(gated_ref.at[pl.ds(0, edge)], halo.at[1], hs.at[1], hr.at[1], at(-1)), halo.at[1]),
    ]

    def start(moves):
        for go, copy, _ in moves:
            @pl.when(inside(go))
            def _():
                copy.start()

    def arrive(moves):
        for go, copy, slot in moves:
            @pl.when(inside(-go))
            def _():
                copy.wait_recv()

            @pl.when(jnp.logical_not(inside(-go)))
            def _():
                slot[...] = jnp.zeros(slot.shape, slot.dtype)

    def left(moves):
        for go, copy, _ in moves:
            @pl.when(inside(go))
            def _():
                copy.wait_send()

    start(steps)
    start(sides)
    own_z = [rcopy(ow_ref, wz.at[d], zs.at[d], zr.at[d], stride[d]) for d in range(half - 1)]
    own_x = rcopy(ow_ref, wx.at[0], ps.at[0], pr.at[0], partner)
    own_x.start()
    for c in own_z:
        c.start()
    arrive(steps)
    for e in range(2):
        for h in range(heads):
            first = near[e, 0, h]
            mixed = dot(first[:, :HEAD], near[e, 1, h])
            pair[e, h, :, :HEAD] = mixed[:, :HEAD].astype(BF16)
            pair[e, h, :, HEAD:] = (mixed[:, HEAD:] + first[:, HEAD:].astype(F32)).astype(BF16)
    hops = []
    for d in range(1, half):
        for e in range(2):
            go = 2 * d if e == 0 else -2 * d
            hops.append((go, rcopy(pair.at[e], far.at[e, d - 1], fs.at[e, d - 1], fr.at[e, d - 1], at(go)), far.at[e, d - 1]))
    start(hops)

    arrive(sides)
    conv_pad[0:edge, :] = halo[0].astype(F32)
    conv_pad[edge : edge + rows, :] = gated_ref[...].astype(F32)
    conv_pad[edge + rows : 2 * edge + rows, :] = halo[1].astype(F32)
    taps = taps_ref[...].astype(F32)
    count = taps.shape[0]
    base = edge - count // 2
    filtered = conv_pad[base : base + rows, :] * taps[0:1, :]
    for tap in range(1, count):
        filtered = filtered + conv_pad[base + tap : base + tap + rows, :] * taps[tap : tap + 1, :]
    sum_col = jnp.sum(filtered, axis=1, keepdims=True)
    square_col = jnp.sum(filtered * filtered, axis=1, keepdims=True)
    lane = lax.broadcasted_iota(jnp.int32, (rows, 128), 1)
    stat[...] = jnp.transpose(jnp.where(lane == 0, sum_col, jnp.where(lane == 1, square_col, 0.0)))[0:8]
    stat_copies = [rcopy(stat, stats.at[d], ss.at[d], sr.at[d], others[d]) for d in range(nt - 1)]
    for c in stat_copies:
        c.start()

    forwards = []
    for d in range(half - 1):
        own_z[d].wait_recv()
        f = rcopy(wz.at[d], wx.at[d + 1], ps.at[d + 1], pr.at[d + 1], partner)
        f.start()
        forwards.append(f)

    for c in stat_copies:
        c.wait_recv()
    whole = stat[...]
    for d in range(nt - 1):
        whole = whole + stats[d]
    back = jnp.transpose(jnp.concatenate([whole, jnp.zeros((120, rows), F32)], axis=0))
    mean = back[:, 0:1] / channels
    second = back[:, 1:2] / channels
    conv_out = jax.nn.silu(
        (filtered - mean) * lax.rsqrt(second - mean * mean + 1e-05) * cgain_ref[...]
    ).astype(BF16)

    arrive(hops)
    delta_heads = []
    for h in range(heads):
        o = within_ref[h]
        for e in range(2):
            entry = jnp.zeros((HEAD, HEAD), F32)
            for d in range(half - 2, -1, -1):
                m = far[e, d, h]
                entry = dot(m[:, :HEAD], entry.astype(BF16)) + m[:, HEAD:].astype(F32)
            m = pair[e, h]
            entry = dot(m[:, :HEAD], entry.astype(BF16)) + m[:, HEAD:].astype(F32)
            o = o + dot(read_ref[e * heads + h], entry.astype(BF16))
        o = o * lax.rsqrt(jnp.mean(jnp.square(o), axis=1, keepdims=True) + 1e-06) * hgain_ref[...]
        delta_heads.append(o.astype(BF16))
    both = jnp.concatenate(delta_heads + [conv_out], axis=1)
    block = ow_ref.shape[1]
    piece = rows // nt

    def emit(src, weights):
        value = dot(both, weights).astype(BF16)
        column = pl.ds(pl.multiple_of(src * block, block), block)
        for p in range(nt):
            part[p, :, column] = value[p * piece : (p + 1) * piece]

    emit(s, ow_ref[...])
    for d in range(half - 1):
        emit(((z + half - 1 - d) % half) * 2 + x, wz[d])
    own_x.wait_recv()
    emit(z * 2 + (1 - x), wx[0])
    for d in range(half - 1):
        forwards[d].wait_recv()
        emit(((z + half - 1 - d) % half) * 2 + (1 - x), wx[d + 1])
    sums = [rcopy(part.at[(t + d) % nt], parts.at[d - 1], rs.at[d - 1], rr.at[d - 1], others[d - 1]) for d in range(1, nt)]
    for c in sums:
        c.start()
    for c in sums:
        c.wait_recv()
    mixed = part[t].astype(F32)
    for d in range(nt - 1):
        mixed = mixed + parts[d].astype(F32)
    out_ref[...] = mixed.astype(BF16)
    left(steps)
    left(sides)
    left(hops)
    for c in own_z + [own_x] + forwards + stat_copies + sums:
        c.wait_send()


def fast_device(
    n, nt,
    inputs, in_gain, query_weight, key_weight, value_weight, beta_weight, decay_weight,
    beta_shift, decay_pace, decay_jolt, head_gain, glu_value_weight, glu_gate_weight,
    conv_kernel, conv_gain, out_delta_weight, out_conv_weight,
):
    rows, part = inputs.shape
    block, width = query_weight.shape
    heads = decay_pace.shape[1]
    half = n // 2
    depth = in_gain.shape[0]
    channels = conv_kernel.shape[1] * nt
    first = lax.axis_index("tp") * heads

    def gate_columns(weight):
        own = lax.dynamic_slice_in_dim(weight, first, heads, 2)
        own = jnp.moveaxis(own, 0, 1).reshape(depth, 2 * heads)
        return jnp.pad(own, ((0, 0), (0, 8 - 2 * heads)))

    gate_weight = jnp.pad(
        jnp.concatenate([gate_columns(beta_weight), gate_columns(decay_weight)], axis=1),
        ((0, 0), (0, 112)),
    )
    pad_rows = ((0, 8 - 2 * heads), (0, 0))
    shift = jnp.pad(
        lax.dynamic_slice_in_dim(beta_shift, first, heads, 1).reshape(2 * heads, 1), pad_rows
    )
    pace = jnp.pad(decay_pace.reshape(2 * heads, rows), pad_rows)
    jolt = jnp.pad(decay_jolt.reshape(2 * heads, rows), pad_rows)
    weights = (query_weight, key_weight, value_weight, glu_value_weight, glu_gate_weight)
    n_in = len(weights)
    dma = pltpu.SemaphoreType.DMA
    qkv, gated, pre = pl.pallas_call(
        functools.partial(project_kernel, n, nt, n_in),
        name="project",
        out_shape=(
            jax.ShapeDtypeStruct((rows, 3 * width), BF16),
            jax.ShapeDtypeStruct((rows, width), BF16),
            jax.ShapeDtypeStruct((rows, 128), F32),
        ),
        in_specs=[VM] * (3 + n_in),
        out_specs=(VM, VM, VM),
        scratch_shapes=[
            pltpu.VMEM((nt - 1, rows, part), BF16),
            pltpu.VMEM((n, rows, block), BF16),
            pltpu.VMEM((rows, n_in * width), F32),
            pltpu.VMEM((half - 1, n_in, block, width), BF16),
            pltpu.VMEM((half, n_in, block, width), BF16),
            dma((nt - 1,)), dma((nt - 1,)),
            dma((half - 1, n_in)), dma((half - 1, n_in)),
            dma((half, n_in)), dma((half, n_in)),
        ],
        compiler_params=pltpu.CompilerParams(collective_id=0, has_side_effects=True),
    )(inputs, in_gain.reshape(n, block), gate_weight, *weights)
    maps, reads, within = pl.pallas_call(
        functools.partial(delta_kernel, heads),
        name="delta",
        out_shape=(
            jax.ShapeDtypeStruct((2 * heads, HEAD, 2 * HEAD), BF16),
            jax.ShapeDtypeStruct((2 * heads, rows, HEAD), BF16),
            jax.ShapeDtypeStruct((heads, rows, HEAD), F32),
        ),
        in_specs=[VM] * 5,
        out_specs=(VM, VM, VM),
    )(qkv, pre, shift, pace, jolt)
    out_weight = jnp.concatenate([out_delta_weight, out_conv_weight], axis=0)
    out_rows, out_block = out_weight.shape
    out_width = out_block * n
    piece = rows // nt
    return pl.pallas_call(
        functools.partial(finish_kernel, n, nt, heads, channels),
        name="finish",
        out_shape=jax.ShapeDtypeStruct((piece, out_width), BF16),
        in_specs=[VM] * 8,
        out_specs=VM,
        scratch_shapes=[
            pltpu.VMEM((2, 2, heads, HEAD, 2 * HEAD), BF16),
            pltpu.VMEM((2, heads, HEAD, 2 * HEAD), BF16),
            pltpu.VMEM((2, half - 1, heads, HEAD, 2 * HEAD), BF16),
            pltpu.VMEM((2, 16, width), BF16),
            pltpu.VMEM((rows + 32, width), F32),
            pltpu.VMEM((8, rows), F32),
            pltpu.VMEM((nt - 1, 8, rows), F32),
            pltpu.VMEM((half - 1, out_rows, out_block), BF16),
            pltpu.VMEM((half, out_rows, out_block), BF16),
            pltpu.VMEM((nt, piece, out_width), BF16),
            pltpu.VMEM((nt - 1, piece, out_width), BF16),
            dma((2, 2)), dma((2, 2)),
            dma((2, half - 1)), dma((2, half - 1)),
            dma((2,)), dma((2,)),
            dma((nt - 1,)), dma((nt - 1,)),
            dma((half - 1,)), dma((half - 1,)),
            dma((half,)), dma((half,)),
            dma((nt - 1,)), dma((nt - 1,)),
        ],
        compiler_params=pltpu.CompilerParams(collective_id=1, has_side_effects=True),
    )(
        maps, reads, within, gated, conv_kernel, conv_gain.reshape(1, width),
        head_gain.reshape(1, HEAD), out_weight,
    )


def device_program(n, nt, *args):
    inputs, query_weight, pace = args[0], args[2], args[8]
    heads = pace.shape[1]
    block, width = query_weight.shape
    suits = (
        n % 2 == 0 and n >= 4 and nt >= 2
        and block % 128 == 0 and width % 128 == 0 and width == heads * HEAD
        and 2 * heads <= 8 and inputs.shape[1] % block == 0 and args[15].shape[1] % 128 == 0
        and args[13].shape[1] == width and V_HEADS == QK_HEADS
        and inputs.shape[0] & (inputs.shape[0] - 1) == 0
        and inputs.shape[0] % 128 == 0 and (inputs.shape[0] // nt) % 16 == 0
        and inputs.shape[0] <= 256 and KERNEL <= 33 and n <= 16
    )
    return fast_device(n, nt, *args) if suits else on_device(*args)


def solution(mesh):
    return jax.shard_map(
        functools.partial(device_program, mesh.shape["sp"], mesh.shape["tp"]),
        mesh=mesh,
        in_specs=(
            P("sp", "tp"),
            P(),
            P("sp", "tp"),
            P("sp", "tp"),
            P("sp", "tp"),
            P(),
            P(),
            P(),
            P(None, "tp", "sp"),
            P(None, "tp", "sp"),
            P(),
            P("sp", "tp"),
            P("sp", "tp"),
            P(None, "tp"),
            P("tp"),
            P("tp", "sp"),
            P("tp", "sp"),
        ),
        out_specs=P(("sp", "tp"), None),
        check_vma=False,
    )
```

```python
import functools

import jax
import jax.numpy as jnp
from jax import lax
from jax.experimental import pallas as pl
from jax.experimental.pallas import tpu as pltpu
from jax.sharding import PartitionSpec as P

HEAD = 128
QK_HEADS = 8
V_HEADS = 8
CONV_CH = 1024
KERNEL = 31
BLOCK = 64


highest = lax.Precision.HIGHEST


def prefix_2(shard, axis, combine, identity, reverse):
    peers, position = (lax.axis_size(axis), lax.axis_index(axis))
    everything = jax.tree.map(
        lambda part, kind: lax.all_gather(part.astype(kind), axis),
        shard,
        (jnp.bfloat16, jnp.bfloat16),
    )
    start = jax.tree.map(
        lambda part, zero: jnp.broadcast_to(jnp.asarray(zero, part.dtype), part.shape),
        shard,
        identity,
    )

    def lap(k, before):
        at = peers - 1 - k if reverse else k
        reached = at > position if reverse else at < position
        new = combine(
            before, jax.tree.map(lambda part, own: part[at].astype(own.dtype), everything, shard)
        )
        return jax.tree.map(lambda a, b: jnp.where(reached, a, b), new, before)

    return lax.fori_loop(0, peers, lap, start)


def padded_2(cells, sides, width):
    for axis, dim in sides:
        count = lax.axis_size(axis)
        ends = count - 1
        head = lax.slice_in_dim(cells, 0, width, axis=dim)
        tail = lax.slice_in_dim(cells, cells.shape[dim] - width, cells.shape[dim], axis=dim)
        cells = jnp.concatenate(
            [
                lax.ppermute(tail, axis, [(i, (i + 1) % count) for i in range(ends)]),
                cells,
                lax.ppermute(head, axis, [((i + 1) % count, i) for i in range(ends)]),
            ],
            axis=dim,
        )
    return cells


def matmul_high(left_side, right_side):
    return jnp.matmul(left_side, right_side, precision=highest)


def unit_lower_inverse(matrix):
    order_size = matrix.shape[-1]
    leading = matrix.shape[:-2]
    inverse = jnp.ones(leading + (order_size, 1, 1), jnp.float32)
    size_now = 1
    while size_now < order_size:
        pair_count = order_size // (2 * size_now)
        halves = inverse.reshape(leading + (pair_count, 2, size_now, size_now))
        upper_inv = halves[..., 0, :, :]
        lower_inv = halves[..., 1, :, :]
        block_grid = matrix.reshape(leading + (pair_count, 2 * size_now, pair_count, 2 * size_now))
        diagonal = jnp.moveaxis(jnp.diagonal(block_grid, axis1=-4, axis2=-2), -1, -3)
        corner = diagonal[..., size_now:, :size_now]
        below = -matmul_high(lower_inv, matmul_high(corner, upper_inv))
        top_half = jnp.concatenate([upper_inv, jnp.zeros_like(below)], axis=-1)
        bottom_half = jnp.concatenate([below, lower_inv], axis=-1)
        inverse = jnp.concatenate([top_half, bottom_half], axis=-2)
        size_now = 2 * size_now
    return inverse.reshape(leading + (order_size, order_size))


def block_terms(queries, key_rows, values, beta_gate, log_decay):
    span = key_rows.shape[-2]
    cumulative = jnp.cumsum(log_decay, axis=-1)
    lower_mask = jnp.tril(jnp.ones((span, span), dtype=bool))
    strict = jnp.tril(jnp.ones((span, span), dtype=bool), -1)
    log_gap = cumulative[..., :, None] - cumulative[..., None, :]
    decay_mask = jnp.where(lower_mask, jnp.exp(jnp.where(lower_mask, log_gap, 0.0)), 0.0)
    key_inner = matmul_high(key_rows, jnp.swapaxes(key_rows, -1, -2))
    below_part = jnp.where(strict, beta_gate[..., :, None] * key_inner * decay_mask, 0.0)
    inverse = unit_lower_inverse(below_part + jnp.eye(span, dtype=jnp.float32))
    fresh = matmul_high(inverse, values * beta_gate[..., None])
    weighted = matmul_high(inverse, key_rows * (beta_gate * jnp.exp(cumulative))[..., None])
    scores = matmul_high(queries, jnp.swapaxes(key_rows, -1, -2)) * decay_mask
    readout = queries * jnp.exp(cumulative)[..., None] - matmul_high(scores, weighted)
    tail_keys = jnp.swapaxes(
        key_rows * jnp.exp(cumulative[..., -1:] - cumulative)[..., None], -1, -2
    )
    identity = jnp.eye(key_rows.shape[-1], dtype=jnp.float32)
    carry_map = jnp.exp(cumulative[..., -1])[..., None, None] * identity - matmul_high(
        tail_keys, weighted
    )
    carry_add = matmul_high(tail_keys, fresh)
    within = matmul_high(scores, fresh)
    return (carry_map, carry_add, readout, within)


def layer_norm_rows(inputs, gain):
    as_float = inputs.astype(jnp.float32)
    mean_row = jnp.mean(as_float, axis=-1, keepdims=True)
    spread = jnp.mean(jnp.square(as_float - mean_row), axis=-1, keepdims=True)
    return ((as_float - mean_row) * lax.rsqrt(spread + 1e-05) * gain).astype(jnp.bfloat16)


def compose(earlier, later):
    return (matmul_high(later[0], earlier[0]), matmul_high(later[0], earlier[1]) + later[1])


def local_maps(queries, key_rows, values, beta_gate, log_decay):
    head_count, length_dev, key_width = queries.shape
    value_width = values.shape[-1]
    block_count = length_dev // BLOCK

    def split_blocks(tensor):
        return tensor.reshape((head_count, block_count, BLOCK) + tensor.shape[2:])

    carry_map, carry_add, readout, within = block_terms(
        split_blocks(queries),
        split_blocks(key_rows),
        split_blocks(values),
        split_blocks(beta_gate),
        split_blocks(log_decay),
    )
    identity = jnp.broadcast_to(
        jnp.eye(key_width, dtype=jnp.float32), (head_count, key_width, key_width)
    )
    nothing = jnp.zeros((head_count, key_width, value_width), jnp.float32)

    def advance(prefix, block_parts):
        prefix_map, prefix_add = prefix
        step_map, step_add, step_read = block_parts
        reach_now = matmul_high(step_read, prefix_map)
        offset_now = matmul_high(step_read, prefix_add)
        return (
            (matmul_high(step_map, prefix_map), matmul_high(step_map, prefix_add) + step_add),
            (reach_now, offset_now),
        )

    moved = (
        jnp.moveaxis(carry_map, 1, 0),
        jnp.moveaxis(carry_add, 1, 0),
        jnp.moveaxis(readout, 1, 0),
    )
    totals, (reach_map, offset) = lax.scan(advance, (identity, nothing), moved)
    reach_map = jnp.moveaxis(reach_map, 0, 1).reshape(head_count, length_dev, key_width)
    offset = (jnp.moveaxis(offset, 0, 1) + within).reshape(head_count, length_dev, value_width)
    return (totals, reach_map, offset)


def on_device(
    inputs,
    in_gain,
    query_weight,
    key_weight,
    value_weight,
    beta_weight,
    decay_weight,
    beta_shift,
    decay_pace,
    decay_jolt,
    head_gain,
    glu_value_weight,
    glu_gate_weight,
    conv_kernel,
    conv_gain,
    out_delta_weight,
    out_conv_weight,
):
    gathered = lax.all_gather(inputs, "tp", axis=1, tiled=True)
    normed = layer_norm_rows(gathered, in_gain)
    row_count = normed.shape[0]

    def add_rows(shard_rows):
        return jnp.dot(normed, shard_rows, preferred_element_type=jnp.float32)

    shards = (
        lax.all_gather(query_weight, "sp", axis=0, tiled=True),
        lax.all_gather(key_weight, "sp", axis=0, tiled=True),
        lax.all_gather(value_weight, "sp", axis=0, tiled=True),
        lax.all_gather(glu_value_weight, "sp", axis=0, tiled=True),
        lax.all_gather(glu_gate_weight, "sp", axis=0, tiled=True),
    )
    projected = tuple((add_rows(shard_rows) for shard_rows in shards))
    delta_sums = projected[:3]
    conv_sums = projected[3:]
    queries, key_proj, value_proj = (summed.astype(jnp.bfloat16) for summed in delta_sums)
    local_heads = value_proj.shape[1] // HEAD
    group_size = V_HEADS // QK_HEADS
    head_first = lax.axis_index("tp") * local_heads

    def by_head(matrix, head_total):
        return jnp.transpose(
            matrix.astype(jnp.float32).reshape(row_count, head_total, HEAD), (1, 0, 2)
        )

    query_heads = jnp.repeat(
        jax.nn.silu(by_head(queries, local_heads // group_size)), group_size, axis=0
    )
    key_heads = jax.nn.silu(by_head(key_proj, local_heads // group_size))
    key_heads = key_heads * lax.rsqrt(
        jnp.sum(jnp.square(key_heads), axis=-1, keepdims=True) + 1e-06
    )
    key_heads = jnp.repeat(key_heads, group_size, axis=0)
    value_heads = by_head(value_proj, local_heads)
    own_beta = lax.dynamic_slice_in_dim(beta_weight, head_first, local_heads, 2)
    own_decay = lax.dynamic_slice_in_dim(decay_weight, head_first, local_heads, 2)
    beta_pre = jnp.einsum("td,edh->eht", normed, own_beta, preferred_element_type=jnp.float32)
    decay_pre = jnp.einsum("td,edh->eht", normed, own_decay, preferred_element_type=jnp.float32)
    own_shift = lax.dynamic_slice_in_dim(beta_shift, head_first, local_heads, 1)
    beta_gate = jax.nn.sigmoid(beta_pre + own_shift[:, :, None])
    log_decay = -decay_pace * jax.nn.softplus(decay_pre) + decay_jolt
    identity = jnp.broadcast_to(jnp.eye(HEAD, dtype=jnp.float32), (local_heads, HEAD, HEAD))
    nothing = jnp.zeros((local_heads, HEAD, HEAD), jnp.float32)
    forward_maps, forward_reach, forward_offset = local_maps(
        query_heads, key_heads, value_heads, beta_gate[0], log_decay[0]
    )
    entry_forward = prefix_2(
        (forward_maps[0], forward_maps[1]), "sp", compose, (identity, nothing), False
    )
    forward_out = matmul_high(forward_reach, entry_forward[1]) + forward_offset
    backward_maps, backward_reach, backward_offset = local_maps(
        jnp.flip(query_heads, 1),
        jnp.flip(key_heads, 1),
        jnp.flip(value_heads, 1),
        jnp.flip(beta_gate[1], 1),
        jnp.flip(log_decay[1], 1),
    )
    entry_backward = prefix_2(
        (backward_maps[0], backward_maps[1]), "sp", compose, (identity, nothing), True
    )
    backward_out = jnp.flip(matmul_high(backward_reach, entry_backward[1]) + backward_offset, 1)
    combined = forward_out + backward_out
    scaled = (
        combined
        * lax.rsqrt(jnp.mean(jnp.square(combined), axis=-1, keepdims=True) + 1e-06)
        * head_gain
    )
    delta_out = (
        jnp.transpose(scaled, (1, 0, 2)).reshape(row_count, local_heads * HEAD).astype(jnp.bfloat16)
    )
    glu_value, glu_gate = (summed.astype(jnp.bfloat16) for summed in conv_sums)
    gated = (glu_value.astype(jnp.float32) * jax.nn.sigmoid(glu_gate.astype(jnp.float32))).astype(
        jnp.bfloat16
    )
    padded = padded_2(gated, (("sp", 0),), KERNEL // 2)
    filtered = jnp.zeros(gated.shape, jnp.float32)
    for tap_index in range(KERNEL):
        filtered = filtered + padded[tap_index : tap_index + row_count].astype(
            jnp.float32
        ) * conv_kernel[tap_index].astype(jnp.float32)
    totals = lax.psum((jnp.sum(filtered, axis=1), jnp.sum(filtered * filtered, axis=1)), "tp")
    mean_row = totals[0][:, None] / CONV_CH
    second = totals[1][:, None] / CONV_CH
    conv_out = jax.nn.silu(
        (filtered - mean_row) * lax.rsqrt(second - mean_row * mean_row + 1e-05) * conv_gain
    ).astype(jnp.bfloat16)
    delta_whole, conv_whole = (
        lax.all_gather(out_delta_weight, "sp", axis=1, tiled=True),
        lax.all_gather(out_conv_weight, "sp", axis=1, tiled=True),
    )
    delta_part = jnp.dot(delta_out, delta_whole, preferred_element_type=jnp.float32)
    conv_part = jnp.dot(conv_out, conv_whole, preferred_element_type=jnp.float32)
    return lax.psum_scatter(
        (delta_part + conv_part).astype(jnp.bfloat16), "tp", scatter_dimension=0, tiled=True
    )


MESH = pl.DeviceIdType.MESH
F32 = jnp.float32
BF16 = jnp.bfloat16
VM = pl.BlockSpec(memory_space=pltpu.VMEM)


def greet(peers):
    barrier = pltpu.get_barrier_semaphore()
    for peer in peers:
        pl.semaphore_signal(barrier, inc=1, device_id=peer, device_id_type=MESH)
    pl.semaphore_wait(barrier, len(peers))


def ring_peers(n):
    s, t = lax.axis_index("sp"), lax.axis_index("tp")
    half = n // 2
    z, x = s // 2, s % 2
    partner = (z * 2 + (1 - x), t)
    stride = [(((z + d) % half) * 2 + x, t) for d in range(1, half)]
    return s, t, z, x, half, partner, stride


def rcopy(src, dst, send, recv, peer):
    return pltpu.make_async_remote_copy(
        src_ref=src, dst_ref=dst, send_sem=send, recv_sem=recv, device_id=peer, device_id_type=MESH
    )


def dot(a, b):
    return jnp.dot(a, b, preferred_element_type=F32)


def dot3(a, b):
    ah, bh = a.astype(BF16), b.astype(BF16)
    al, bl = (a - ah.astype(F32)).astype(BF16), (b - bh.astype(F32)).astype(BF16)
    return dot(ah, bh) + (dot(ah, bl) + dot(al, bh))


def layer_kernel(n, nt, heads, channels, *refs):
    (x_ref, gain_ref, wg_ref, shift_ref, pace_ref, jolt_ref, taps_ref, cgain_ref, hgain_ref) = refs[:9]
    w_refs = refs[9:16]
    out_ref = refs[16]
    (
        xbuf, normed, acc, wz, wx,
        maps, reads, near, pair, far, halo, edges, conv_pad, stat, stats, part, parts,
        xs, xr, zs, zr, ps, pr,
        ns, nr, fs, fr, hs, hr, ss, sr, rs, rr,
    ) = refs[17:]
    s, t, z, x, half, partner, stride = ring_peers(n)
    others = [(s, (t + d) % nt) for d in range(1, nt)]
    greet(others + [((s + d) % n, t) for d in range(1, n)])
    order = list(range(half - 1))
    n_w = len(w_refs)
    n_in = n_w - 2
    rows, width_x = x_ref.shape
    block, width = w_refs[0].shape

    def came(d, side):
        return ((z + half - 1 - d) % half) * 2 + side

    x_copies = [rcopy(x_ref, xbuf.at[d], xs.at[d], xr.at[d], others[d]) for d in range(nt - 1)]
    for c in x_copies:
        c.start()
    own_x = [rcopy(w_refs[w], wx.at[0, w], ps.at[0, w], pr.at[0, w], partner) for w in range(n_w)]
    own_z = [
        [rcopy(w_refs[w], wz.at[d, w], zs.at[d, w], zr.at[d, w], stride[d]) for d in order]
        for w in range(n_w)
    ]
    forwards = [
        [rcopy(wz.at[d, w], wx.at[d + 1, w], ps.at[d + 1, w], pr.at[d + 1, w], partner) for d in order]
        for w in range(n_w)
    ]

    def send_z(w):
        for d in order:
            own_z[w][d].start()

    for w in range(3):
        send_z(w)
        own_x[w].start()
    for w in range(3, n_w):
        send_z(w)
    for c in x_copies:
        c.wait_recv()
    per = width_x // block
    depth = width_x * nt
    chunks = [(t, x_ref)] + [((t + nt - 1 - d) % nt, xbuf.at[d]) for d in range(nt - 1)]
    mean = sum(jnp.sum(r[...].astype(F32), axis=1, keepdims=True) for _, r in chunks) / depth
    var = (
        sum(jnp.sum(jnp.square(r[...].astype(F32) - mean), axis=1, keepdims=True) for _, r in chunks)
        / depth
    )
    inv = lax.rsqrt(var + 1e-05)
    for src, r in chunks:
        y = (r[...].astype(F32) - mean) * inv
        for p in range(per):
            b = src * per + p
            g = gain_ref[:, pl.ds(pl.multiple_of(b * block, block), block)]
            normed[b] = (y[:, p * block : (p + 1) * block] * g).astype(BF16)
    pre = dot(normed[0], wg_ref[0:block, :])
    for b in range(1, n):
        pre = pre + dot(normed[b], wg_ref[b * block : (b + 1) * block, :])

    def relay(w):
        for d in order:
            own_z[w][d].wait_recv()
            forwards[w][d].start()

    def near_half(w):
        value = dot(normed[s], w_refs[w][...])
        for d in order:
            value = value + dot(normed[came(d, x)], wz[d, w])
        acc[w] = value

    def far_half(w):
        own_x[w].wait_recv()
        value = acc[w] + dot(normed[z * 2 + (1 - x)], wx[0, w])
        for d in order:
            forwards[w][d].wait_recv()
            value = value + dot(normed[came(d, 1 - x)], wx[d + 1, w])
        acc[w] = value

    for w in range(3):
        relay(w)
        near_half(w)
    own_x[3].start()
    own_x[4].start()
    for w in range(3):
        far_half(w)

    span = rows
    pre_rows = jnp.transpose(pre)
    which = lax.broadcasted_iota(jnp.int32, (8, span), 0)
    shift_lane = lax.broadcasted_iota(jnp.int32, shift_ref.shape, 1)
    shift_rows = jnp.zeros((8, span), F32)
    pace_rows = jnp.zeros((8, span), F32)
    jolt_rows = jnp.zeros((8, span), F32)
    for h in range(heads):
        mine = jnp.sum(
            jnp.where(shift_lane == t * heads + h, shift_ref[...], 0.0), axis=1, keepdims=True
        )
        for e in range(2):
            here = which == e * heads + h
            shift_rows = jnp.where(here, mine[e : e + 1, :], shift_rows)
            pace_rows = jnp.where(here, pace_ref[e, h : h + 1, :], pace_rows)
            jolt_rows = jnp.where(here, jolt_ref[e, h : h + 1, :], jolt_rows)
    beta = jax.nn.sigmoid(pre_rows[0:8] + shift_rows)
    log_decay = -pace_rows * jax.nn.softplus(pre_rows[8:16]) + jolt_rows
    i = lax.broadcasted_iota(jnp.int32, (span, span), 0)
    j = lax.broadcasted_iota(jnp.int32, (span, span), 1)
    high = lax.Precision.HIGHEST
    upto = jnp.dot(log_decay, (i <= j).astype(F32), precision=high, preferred_element_type=F32)
    onto = jnp.dot(log_decay, (i >= j).astype(F32), precision=high, preferred_element_type=F32)
    cum = jnp.where(which < heads, upto, onto)
    cols = jnp.transpose(jnp.concatenate([beta, cum, jnp.zeros((112, span), F32)], axis=0))
    eye = (i == j).astype(F32)
    eye_head = (
        lax.broadcasted_iota(jnp.int32, (HEAD, HEAD), 0)
        == lax.broadcasted_iota(jnp.int32, (HEAD, HEAD), 1)
    ).astype(F32)
    level = i ^ j
    within = []
    for h in range(heads):
        lo = h * HEAD
        q = jax.nn.silu(acc[0, :, lo : lo + HEAD].astype(BF16).astype(F32))
        k = jax.nn.silu(acc[1, :, lo : lo + HEAD].astype(BF16).astype(F32))
        k = k * lax.rsqrt(jnp.sum(jnp.square(k), axis=1, keepdims=True) + 1e-06)
        v = acc[2, :, lo : lo + HEAD].astype(BF16).astype(F32)
        kt = jnp.transpose(k)
        kk = dot3(k, kt)
        qk = dot(q.astype(BF16), kt.astype(BF16))
        total = jnp.zeros((span, HEAD), F32)
        for e in range(2):
            c = e * heads + h
            beta_col = cols[:, c : c + 1]
            cum_col = cols[:, 8 + c : 9 + c]
            cum_row = cum[c : c + 1, :]
            keep = (i >= j) if e == 0 else (i <= j)
            gap = jnp.exp(jnp.where(keep, cum_col - cum_row, 0.0))
            decay = jnp.where(keep, gap, 0.0)
            below = jnp.where(i == j, 0.0, beta_col * kk * decay)
            inverse = eye - jnp.where(level < 2, below, 0.0)
            size = 2
            while size < span:
                corner = jnp.where((level >= size) & (level < 2 * size), below, 0.0)
                inverse = inverse - dot3(inverse, dot3(corner, inverse))
                size = 2 * size
            grown = jnp.exp(cum_col)
            rhs = jnp.concatenate([v * beta_col, k * (beta_col * grown)], axis=1)
            solved = dot3(inverse, rhs)
            solved_b = solved.astype(BF16)
            out = dot((qk * decay).astype(BF16), solved_b)
            total = total + out[:, :HEAD]
            reads[c] = (q * grown - out[:, HEAD:]).astype(BF16)
            end = cum[c : c + 1, span - 1 : span] if e == 0 else cum[c : c + 1, 0:1]
            tail = jnp.transpose(k * jnp.exp(end - cum_col))
            state = dot3(tail, solved)
            maps[c, :, :HEAD] = (jnp.exp(end) * eye_head - state[:, HEAD:]).astype(BF16)
            maps[c, :, HEAD:] = state[:, :HEAD].astype(BF16)
        within.append(total)
        if h < 2:
            relay(3 + h)
    for w in range(3 + min(heads, 2), n_in):
        relay(w)

    edge = 16

    def at(offset):
        return ((s + offset + n) % n, t)

    def inside(offset):
        return (s < n - offset) if offset > 0 else (s >= -offset)

    def start(moves):
        for go, copy, _ in moves:
            @pl.when(inside(go))
            def _():
                copy.start()

    def arrive(moves):
        for go, copy, slot in moves:
            @pl.when(inside(-go))
            def _():
                copy.wait_recv()

            @pl.when(jnp.logical_not(inside(-go)))
            def _():
                slot[...] = jnp.zeros(slot.shape, slot.dtype)

    def left(moves):
        for go, copy, _ in moves:
            @pl.when(inside(go))
            def _():
                copy.wait_send()

    steps = []
    for d in (1, 2):
        for e in range(2):
            go = d if e == 0 else -d
            slot = near.at[e, d - 1]
            steps.append((go, rcopy(maps.at[pl.ds(e * heads, heads)], slot, ns.at[e, d - 1], nr.at[e, d - 1], at(go)), slot))
    start(steps)

    for w in range(3, n_in):
        near_half(w)
    for w in range(3, n_in):
        far_half(w)
    glu_value = acc[3].astype(BF16).astype(F32)
    glu_gate = acc[4].astype(BF16).astype(F32)
    gated = (glu_value * jax.nn.sigmoid(glu_gate)).astype(BF16)
    edges[0] = gated[0:edge]
    edges[1] = gated[rows - edge : rows]
    sides = [
        (1, rcopy(edges.at[1], halo.at[0], hs.at[0], hr.at[0], at(1)), halo.at[0]),
        (-1, rcopy(edges.at[0], halo.at[1], hs.at[1], hr.at[1], at(-1)), halo.at[1]),
    ]
    start(sides)
    arrive(steps)
    for e in range(2):
        for h in range(heads):
            first = near[e, 0, h]
            mixed = dot(first[:, :HEAD], near[e, 1, h])
            pair[e, h, :, :HEAD] = mixed[:, :HEAD].astype(BF16)
            pair[e, h, :, HEAD:] = (mixed[:, HEAD:] + first[:, HEAD:].astype(F32)).astype(BF16)
    hops = []
    for d in range(1, half):
        for e in range(2):
            go = 2 * d if e == 0 else -2 * d
            slot = far.at[e, d - 1]
            hops.append((go, rcopy(pair.at[e], slot, fs.at[e, d - 1], fr.at[e, d - 1], at(go)), slot))
    start(hops)
    for w in range(n_in, n_w):
        own_x[w].start()
    relay(n_in)

    conv_pad[edge : edge + rows, :] = gated.astype(F32)
    arrive(sides)
    conv_pad[0:edge, :] = halo[0].astype(F32)
    conv_pad[edge + rows : 2 * edge + rows, :] = halo[1].astype(F32)
    taps = taps_ref[...].astype(F32)
    count = taps.shape[0]
    base = edge - count // 2
    filtered = conv_pad[base : base + rows, :] * taps[0:1, :]
    for tap in range(1, count):
        filtered = filtered + conv_pad[base + tap : base + tap + rows, :] * taps[tap : tap + 1, :]
    sum_col = jnp.sum(filtered, axis=1, keepdims=True)
    square_col = jnp.sum(filtered * filtered, axis=1, keepdims=True)
    lane = lax.broadcasted_iota(jnp.int32, (rows, 128), 1)
    stat[...] = jnp.transpose(jnp.where(lane == 0, sum_col, jnp.where(lane == 1, square_col, 0.0)))[0:8]
    stat_copies = [rcopy(stat, stats.at[d], ss.at[d], sr.at[d], others[d]) for d in range(nt - 1)]
    for c in stat_copies:
        c.start()
    for w in range(n_in + 1, n_w):
        relay(w)
    for c in stat_copies:
        c.wait_recv()
    whole = stat[...]
    for d in range(nt - 1):
        whole = whole + stats[d]
    back = jnp.transpose(jnp.concatenate([whole, jnp.zeros((120, rows), F32)], axis=0))
    mean = back[:, 0:1] / channels
    second = back[:, 1:2] / channels
    conv_out = jax.nn.silu(
        (filtered - mean) * lax.rsqrt(second - mean * mean + 1e-05) * cgain_ref[...]
    ).astype(BF16)

    arrive(hops)
    delta_heads = []
    for h in range(heads):
        o = within[h]
        for e in range(2):
            entry = jnp.zeros((HEAD, HEAD), F32)
            for d in range(half - 2, -1, -1):
                m = far[e, d, h]
                entry = dot(m[:, :HEAD], entry.astype(BF16)) + m[:, HEAD:].astype(F32)
            m = pair[e, h]
            entry = dot(m[:, :HEAD], entry.astype(BF16)) + m[:, HEAD:].astype(F32)
            o = o + dot(reads[e * heads + h], entry.astype(BF16))
        o = o * lax.rsqrt(jnp.mean(jnp.square(o), axis=1, keepdims=True) + 1e-06) * hgain_ref[...]
        delta_heads.append(o.astype(BF16))
    delta_out = jnp.concatenate(delta_heads, axis=1)
    piece = rows // nt
    sums = []

    def emit(first, second):
        at_block = len(sums)
        value = (dot(delta_out, first) + dot(conv_out, second)).astype(BF16)
        for p in range(nt):
            part[at_block, p] = value[p * piece : (p + 1) * piece]
        copies = [
            rcopy(part.at[at_block, (t + d) % nt], parts.at[d - 1, at_block], rs.at[d - 1, at_block], rr.at[d - 1, at_block], others[d - 1])
            for d in range(1, nt)
        ]
        for c in copies:
            c.start()
        sums.append(copies)

    sources = [s]
    emit(w_refs[n_in][...], w_refs[n_in + 1][...])
    for d in order:
        sources.append(came(d, x))
        emit(wz[d, n_in], wz[d, n_in + 1])
    sources.append(z * 2 + (1 - x))
    own_x[n_in].wait_recv()
    own_x[n_in + 1].wait_recv()
    emit(wx[0, n_in], wx[0, n_in + 1])
    for d in order:
        forwards[n_in][d].wait_recv()
        forwards[n_in + 1][d].wait_recv()
        sources.append(came(d, 1 - x))
        emit(wx[d + 1, n_in], wx[d + 1, n_in + 1])
    out_block = w_refs[n_in].shape[1]
    for b in range(n):
        mixed = part[b, t].astype(F32)
        for d in range(nt - 1):
            sums[b][d].wait_recv()
            mixed = mixed + parts[d, b].astype(F32)
        out_ref[:, pl.ds(pl.multiple_of(sources[b] * out_block, out_block), out_block)] = mixed.astype(BF16)
    left(steps)
    left(sides)
    left(hops)
    for group in own_z + forwards + sums + [x_copies, own_x, stat_copies]:
        for c in group:
            c.wait_send()


def fast_device(
    n, nt,
    inputs, in_gain, query_weight, key_weight, value_weight, beta_weight, decay_weight,
    beta_shift, decay_pace, decay_jolt, head_gain, glu_value_weight, glu_gate_weight,
    conv_kernel, conv_gain, out_delta_weight, out_conv_weight,
):
    rows, width_x = inputs.shape
    block, width = query_weight.shape
    heads = decay_pace.shape[1]
    half = n // 2
    depth = in_gain.shape[0]
    channels = conv_kernel.shape[1] * nt
    first = lax.axis_index("tp") * heads

    def gate_columns(weight):
        own = lax.dynamic_slice_in_dim(weight, first, heads, 2)
        own = jnp.moveaxis(own, 0, 1).reshape(depth, 2 * heads)
        return jnp.pad(own, ((0, 0), (0, 8 - 2 * heads)))

    gate_weight = jnp.pad(
        jnp.concatenate([gate_columns(beta_weight), gate_columns(decay_weight)], axis=1),
        ((0, 0), (0, 112)),
    )
    weights = (
        query_weight, key_weight, value_weight, glu_value_weight, glu_gate_weight,
        out_delta_weight, out_conv_weight,
    )
    n_w = len(weights)
    out_block = out_delta_weight.shape[1]
    piece = rows // nt
    dma = pltpu.SemaphoreType.DMA
    return pl.pallas_call(
        functools.partial(layer_kernel, n, nt, heads, channels),
        name="layer",
        out_shape=jax.ShapeDtypeStruct((piece, out_block * n), BF16),
        in_specs=[VM] * (9 + n_w),
        out_specs=VM,
        scratch_shapes=[
            pltpu.VMEM((nt - 1, rows, width_x), BF16),
            pltpu.VMEM((n, rows, block), BF16),
            pltpu.VMEM((n_w - 2, rows, width), F32),
            pltpu.VMEM((half - 1, n_w, block, width), BF16),
            pltpu.VMEM((half, n_w, block, width), BF16),
            pltpu.VMEM((2 * heads, HEAD, 2 * HEAD), BF16),
            pltpu.VMEM((2 * heads, rows, HEAD), BF16),
            pltpu.VMEM((2, 2, heads, HEAD, 2 * HEAD), BF16),
            pltpu.VMEM((2, heads, HEAD, 2 * HEAD), BF16),
            pltpu.VMEM((2, half - 1, heads, HEAD, 2 * HEAD), BF16),
            pltpu.VMEM((2, 16, width), BF16),
            pltpu.VMEM((2, 16, width), BF16),
            pltpu.VMEM((rows + 32, width), F32),
            pltpu.VMEM((8, rows), F32),
            pltpu.VMEM((nt - 1, 8, rows), F32),
            pltpu.VMEM((n, nt, piece, out_block), BF16),
            pltpu.VMEM((nt - 1, n, piece, out_block), BF16),
            dma((nt - 1,)), dma((nt - 1,)),
            dma((half - 1, n_w)), dma((half - 1, n_w)),
            dma((half, n_w)), dma((half, n_w)),
            dma((2, 2)), dma((2, 2)),
            dma((2, half - 1)), dma((2, half - 1)),
            dma((2,)), dma((2,)),
            dma((nt - 1,)), dma((nt - 1,)),
            dma((nt - 1, n)), dma((nt - 1, n)),
        ],
        compiler_params=pltpu.CompilerParams(collective_id=0, has_side_effects=True),
    )(
        inputs, in_gain.reshape(1, depth), gate_weight, beta_shift, decay_pace, decay_jolt,
        conv_kernel, conv_gain.reshape(1, width), head_gain.reshape(1, HEAD), *weights,
    )


def device_program(n, nt, *args):
    inputs, query_weight, pace = args[0], args[2], args[8]
    heads = pace.shape[1]
    block, width = query_weight.shape
    suits = (
        n % 2 == 0 and n >= 4 and nt >= 2
        and block % 128 == 0 and width % 128 == 0 and width == heads * HEAD
        and 2 * heads <= 8 and inputs.shape[1] % block == 0 and args[15].shape[1] % 128 == 0
        and args[13].shape[1] == width and args[15].shape == (block, width) and V_HEADS == QK_HEADS
        and inputs.shape[0] & (inputs.shape[0] - 1) == 0
        and inputs.shape[0] % 128 == 0 and (inputs.shape[0] // nt) % 16 == 0
        and inputs.shape[0] <= 256 and KERNEL <= 33 and n <= 16
    )
    return fast_device(n, nt, *args) if suits else on_device(*args)


def solution(mesh):
    return jax.shard_map(
        functools.partial(device_program, mesh.shape["sp"], mesh.shape["tp"]),
        mesh=mesh,
        in_specs=(
            P("sp", "tp"),
            P(),
            P("sp", "tp"),
            P("sp", "tp"),
            P("sp", "tp"),
            P(),
            P(),
            P(),
            P(None, "tp", "sp"),
            P(None, "tp", "sp"),
            P(),
            P("sp", "tp"),
            P("sp", "tp"),
            P(None, "tp"),
            P("tp"),
            P("tp", "sp"),
            P("tp", "sp"),
        ),
        out_specs=P(("sp", "tp"), None),
        check_vma=False,
    )
```

```python
import functools

import jax
import jax.numpy as jnp
from jax import lax
from jax.experimental import pallas as pl
from jax.experimental.pallas import tpu as pltpu
from jax.sharding import PartitionSpec as P

HEAD = 128
QK_HEADS = 8
V_HEADS = 8
CONV_CH = 1024
KERNEL = 31
BLOCK = 64


highest = lax.Precision.HIGHEST


def prefix_2(shard, axis, combine, identity, reverse):
    peers, position = (lax.axis_size(axis), lax.axis_index(axis))
    everything = jax.tree.map(
        lambda part, kind: lax.all_gather(part.astype(kind), axis),
        shard,
        (jnp.bfloat16, jnp.bfloat16),
    )
    start = jax.tree.map(
        lambda part, zero: jnp.broadcast_to(jnp.asarray(zero, part.dtype), part.shape),
        shard,
        identity,
    )

    def lap(k, before):
        at = peers - 1 - k if reverse else k
        reached = at > position if reverse else at < position
        new = combine(
            before, jax.tree.map(lambda part, own: part[at].astype(own.dtype), everything, shard)
        )
        return jax.tree.map(lambda a, b: jnp.where(reached, a, b), new, before)

    return lax.fori_loop(0, peers, lap, start)


def padded_2(cells, sides, width):
    for axis, dim in sides:
        count = lax.axis_size(axis)
        ends = count - 1
        head = lax.slice_in_dim(cells, 0, width, axis=dim)
        tail = lax.slice_in_dim(cells, cells.shape[dim] - width, cells.shape[dim], axis=dim)
        cells = jnp.concatenate(
            [
                lax.ppermute(tail, axis, [(i, (i + 1) % count) for i in range(ends)]),
                cells,
                lax.ppermute(head, axis, [((i + 1) % count, i) for i in range(ends)]),
            ],
            axis=dim,
        )
    return cells


def matmul_high(left_side, right_side):
    return jnp.matmul(left_side, right_side, precision=highest)


def unit_lower_inverse(matrix):
    order_size = matrix.shape[-1]
    leading = matrix.shape[:-2]
    inverse = jnp.ones(leading + (order_size, 1, 1), jnp.float32)
    size_now = 1
    while size_now < order_size:
        pair_count = order_size // (2 * size_now)
        halves = inverse.reshape(leading + (pair_count, 2, size_now, size_now))
        upper_inv = halves[..., 0, :, :]
        lower_inv = halves[..., 1, :, :]
        block_grid = matrix.reshape(leading + (pair_count, 2 * size_now, pair_count, 2 * size_now))
        diagonal = jnp.moveaxis(jnp.diagonal(block_grid, axis1=-4, axis2=-2), -1, -3)
        corner = diagonal[..., size_now:, :size_now]
        below = -matmul_high(lower_inv, matmul_high(corner, upper_inv))
        top_half = jnp.concatenate([upper_inv, jnp.zeros_like(below)], axis=-1)
        bottom_half = jnp.concatenate([below, lower_inv], axis=-1)
        inverse = jnp.concatenate([top_half, bottom_half], axis=-2)
        size_now = 2 * size_now
    return inverse.reshape(leading + (order_size, order_size))


def block_terms(queries, key_rows, values, beta_gate, log_decay):
    span = key_rows.shape[-2]
    cumulative = jnp.cumsum(log_decay, axis=-1)
    lower_mask = jnp.tril(jnp.ones((span, span), dtype=bool))
    strict = jnp.tril(jnp.ones((span, span), dtype=bool), -1)
    log_gap = cumulative[..., :, None] - cumulative[..., None, :]
    decay_mask = jnp.where(lower_mask, jnp.exp(jnp.where(lower_mask, log_gap, 0.0)), 0.0)
    key_inner = matmul_high(key_rows, jnp.swapaxes(key_rows, -1, -2))
    below_part = jnp.where(strict, beta_gate[..., :, None] * key_inner * decay_mask, 0.0)
    inverse = unit_lower_inverse(below_part + jnp.eye(span, dtype=jnp.float32))
    fresh = matmul_high(inverse, values * beta_gate[..., None])
    weighted = matmul_high(inverse, key_rows * (beta_gate * jnp.exp(cumulative))[..., None])
    scores = matmul_high(queries, jnp.swapaxes(key_rows, -1, -2)) * decay_mask
    readout = queries * jnp.exp(cumulative)[..., None] - matmul_high(scores, weighted)
    tail_keys = jnp.swapaxes(
        key_rows * jnp.exp(cumulative[..., -1:] - cumulative)[..., None], -1, -2
    )
    identity = jnp.eye(key_rows.shape[-1], dtype=jnp.float32)
    carry_map = jnp.exp(cumulative[..., -1])[..., None, None] * identity - matmul_high(
        tail_keys, weighted
    )
    carry_add = matmul_high(tail_keys, fresh)
    within = matmul_high(scores, fresh)
    return (carry_map, carry_add, readout, within)


def layer_norm_rows(inputs, gain):
    as_float = inputs.astype(jnp.float32)
    mean_row = jnp.mean(as_float, axis=-1, keepdims=True)
    spread = jnp.mean(jnp.square(as_float - mean_row), axis=-1, keepdims=True)
    return ((as_float - mean_row) * lax.rsqrt(spread + 1e-05) * gain).astype(jnp.bfloat16)


def compose(earlier, later):
    return (matmul_high(later[0], earlier[0]), matmul_high(later[0], earlier[1]) + later[1])


def local_maps(queries, key_rows, values, beta_gate, log_decay):
    head_count, length_dev, key_width = queries.shape
    value_width = values.shape[-1]
    block_count = length_dev // BLOCK

    def split_blocks(tensor):
        return tensor.reshape((head_count, block_count, BLOCK) + tensor.shape[2:])

    carry_map, carry_add, readout, within = block_terms(
        split_blocks(queries),
        split_blocks(key_rows),
        split_blocks(values),
        split_blocks(beta_gate),
        split_blocks(log_decay),
    )
    identity = jnp.broadcast_to(
        jnp.eye(key_width, dtype=jnp.float32), (head_count, key_width, key_width)
    )
    nothing = jnp.zeros((head_count, key_width, value_width), jnp.float32)

    def advance(prefix, block_parts):
        prefix_map, prefix_add = prefix
        step_map, step_add, step_read = block_parts
        reach_now = matmul_high(step_read, prefix_map)
        offset_now = matmul_high(step_read, prefix_add)
        return (
            (matmul_high(step_map, prefix_map), matmul_high(step_map, prefix_add) + step_add),
            (reach_now, offset_now),
        )

    moved = (
        jnp.moveaxis(carry_map, 1, 0),
        jnp.moveaxis(carry_add, 1, 0),
        jnp.moveaxis(readout, 1, 0),
    )
    totals, (reach_map, offset) = lax.scan(advance, (identity, nothing), moved)
    reach_map = jnp.moveaxis(reach_map, 0, 1).reshape(head_count, length_dev, key_width)
    offset = (jnp.moveaxis(offset, 0, 1) + within).reshape(head_count, length_dev, value_width)
    return (totals, reach_map, offset)


def on_device(
    inputs,
    in_gain,
    query_weight,
    key_weight,
    value_weight,
    beta_weight,
    decay_weight,
    beta_shift,
    decay_pace,
    decay_jolt,
    head_gain,
    glu_value_weight,
    glu_gate_weight,
    conv_kernel,
    conv_gain,
    out_delta_weight,
    out_conv_weight,
):
    gathered = lax.all_gather(inputs, "tp", axis=1, tiled=True)
    normed = layer_norm_rows(gathered, in_gain)
    row_count = normed.shape[0]

    def add_rows(shard_rows):
        return jnp.dot(normed, shard_rows, preferred_element_type=jnp.float32)

    shards = (
        lax.all_gather(query_weight, "sp", axis=0, tiled=True),
        lax.all_gather(key_weight, "sp", axis=0, tiled=True),
        lax.all_gather(value_weight, "sp", axis=0, tiled=True),
        lax.all_gather(glu_value_weight, "sp", axis=0, tiled=True),
        lax.all_gather(glu_gate_weight, "sp", axis=0, tiled=True),
    )
    projected = tuple((add_rows(shard_rows) for shard_rows in shards))
    delta_sums = projected[:3]
    conv_sums = projected[3:]
    queries, key_proj, value_proj = (summed.astype(jnp.bfloat16) for summed in delta_sums)
    local_heads = value_proj.shape[1] // HEAD
    group_size = V_HEADS // QK_HEADS
    head_first = lax.axis_index("tp") * local_heads

    def by_head(matrix, head_total):
        return jnp.transpose(
            matrix.astype(jnp.float32).reshape(row_count, head_total, HEAD), (1, 0, 2)
        )

    query_heads = jnp.repeat(
        jax.nn.silu(by_head(queries, local_heads // group_size)), group_size, axis=0
    )
    key_heads = jax.nn.silu(by_head(key_proj, local_heads // group_size))
    key_heads = key_heads * lax.rsqrt(
        jnp.sum(jnp.square(key_heads), axis=-1, keepdims=True) + 1e-06
    )
    key_heads = jnp.repeat(key_heads, group_size, axis=0)
    value_heads = by_head(value_proj, local_heads)
    own_beta = lax.dynamic_slice_in_dim(beta_weight, head_first, local_heads, 2)
    own_decay = lax.dynamic_slice_in_dim(decay_weight, head_first, local_heads, 2)
    beta_pre = jnp.einsum("td,edh->eht", normed, own_beta, preferred_element_type=jnp.float32)
    decay_pre = jnp.einsum("td,edh->eht", normed, own_decay, preferred_element_type=jnp.float32)
    own_shift = lax.dynamic_slice_in_dim(beta_shift, head_first, local_heads, 1)
    beta_gate = jax.nn.sigmoid(beta_pre + own_shift[:, :, None])
    log_decay = -decay_pace * jax.nn.softplus(decay_pre) + decay_jolt
    identity = jnp.broadcast_to(jnp.eye(HEAD, dtype=jnp.float32), (local_heads, HEAD, HEAD))
    nothing = jnp.zeros((local_heads, HEAD, HEAD), jnp.float32)
    forward_maps, forward_reach, forward_offset = local_maps(
        query_heads, key_heads, value_heads, beta_gate[0], log_decay[0]
    )
    entry_forward = prefix_2(
        (forward_maps[0], forward_maps[1]), "sp", compose, (identity, nothing), False
    )
    forward_out = matmul_high(forward_reach, entry_forward[1]) + forward_offset
    backward_maps, backward_reach, backward_offset = local_maps(
        jnp.flip(query_heads, 1),
        jnp.flip(key_heads, 1),
        jnp.flip(value_heads, 1),
        jnp.flip(beta_gate[1], 1),
        jnp.flip(log_decay[1], 1),
    )
    entry_backward = prefix_2(
        (backward_maps[0], backward_maps[1]), "sp", compose, (identity, nothing), True
    )
    backward_out = jnp.flip(matmul_high(backward_reach, entry_backward[1]) + backward_offset, 1)
    combined = forward_out + backward_out
    scaled = (
        combined
        * lax.rsqrt(jnp.mean(jnp.square(combined), axis=-1, keepdims=True) + 1e-06)
        * head_gain
    )
    delta_out = (
        jnp.transpose(scaled, (1, 0, 2)).reshape(row_count, local_heads * HEAD).astype(jnp.bfloat16)
    )
    glu_value, glu_gate = (summed.astype(jnp.bfloat16) for summed in conv_sums)
    gated = (glu_value.astype(jnp.float32) * jax.nn.sigmoid(glu_gate.astype(jnp.float32))).astype(
        jnp.bfloat16
    )
    padded = padded_2(gated, (("sp", 0),), KERNEL // 2)
    filtered = jnp.zeros(gated.shape, jnp.float32)
    for tap_index in range(KERNEL):
        filtered = filtered + padded[tap_index : tap_index + row_count].astype(
            jnp.float32
        ) * conv_kernel[tap_index].astype(jnp.float32)
    totals = lax.psum((jnp.sum(filtered, axis=1), jnp.sum(filtered * filtered, axis=1)), "tp")
    mean_row = totals[0][:, None] / CONV_CH
    second = totals[1][:, None] / CONV_CH
    conv_out = jax.nn.silu(
        (filtered - mean_row) * lax.rsqrt(second - mean_row * mean_row + 1e-05) * conv_gain
    ).astype(jnp.bfloat16)
    delta_whole, conv_whole = (
        lax.all_gather(out_delta_weight, "sp", axis=1, tiled=True),
        lax.all_gather(out_conv_weight, "sp", axis=1, tiled=True),
    )
    delta_part = jnp.dot(delta_out, delta_whole, preferred_element_type=jnp.float32)
    conv_part = jnp.dot(conv_out, conv_whole, preferred_element_type=jnp.float32)
    return lax.psum_scatter(
        (delta_part + conv_part).astype(jnp.bfloat16), "tp", scatter_dimension=0, tiled=True
    )


MESH = pl.DeviceIdType.MESH
F32 = jnp.float32
BF16 = jnp.bfloat16
VM = pl.BlockSpec(memory_space=pltpu.VMEM)


def greet(peers):
    barrier = pltpu.get_barrier_semaphore()
    for peer in peers:
        pl.semaphore_signal(barrier, inc=1, device_id=peer, device_id_type=MESH)
    pl.semaphore_wait(barrier, len(peers))


def ring_peers(n):
    s, t = lax.axis_index("sp"), lax.axis_index("tp")
    half = n // 2
    z, x = s // 2, s % 2
    partner = (z * 2 + (1 - x), t)
    stride = [(((z + d) % half) * 2 + x, t) for d in range(1, half)]
    return s, t, z, x, half, partner, stride


def rcopy(src, dst, send, recv, peer):
    return pltpu.make_async_remote_copy(
        src_ref=src, dst_ref=dst, send_sem=send, recv_sem=recv, device_id=peer, device_id_type=MESH
    )


def dot(a, b):
    return jnp.dot(a, b, preferred_element_type=F32)


def dot3(a, b):
    ah, bh = a.astype(BF16), b.astype(BF16)
    al, bl = (a - ah.astype(F32)).astype(BF16), (b - bh.astype(F32)).astype(BF16)
    return dot(ah, bh) + (dot(ah, bl) + dot(al, bh))


def layer_kernel(n, nt, heads, channels, *refs):
    (x_ref, gain_ref, wg_ref, shift_ref, pace_ref, jolt_ref, taps_ref, cgain_ref, hgain_ref) = refs[:9]
    w_refs = refs[9:16]
    out_ref = refs[16]
    (
        xbuf, normed, acc, wz, wx,
        maps, reads, near, pair, far, halo, edges, conv_pad, stat, stats, part, parts,
        xs, xr, zs, zr, ps, pr,
        ns, nr, fs, fr, hs, hr, ss, sr, rs, rr,
    ) = refs[17:]
    s, t, z, x, half, partner, stride = ring_peers(n)
    others = [(s, (t + d) % nt) for d in range(1, nt)]
    greet(others + [((s + d) % n, t) for d in range(1, n)])
    order = list(range(half - 1))
    n_w = len(w_refs)
    n_in = n_w - 2
    rows, width_x = x_ref.shape
    block, width = w_refs[0].shape

    def came(d, side):
        return ((z + half - 1 - d) % half) * 2 + side

    x_copies = [rcopy(x_ref, xbuf.at[d], xs.at[d], xr.at[d], others[d]) for d in range(nt - 1)]
    for c in x_copies:
        c.start()
    own_x = [rcopy(w_refs[w], wx.at[0, w], ps.at[0, w], pr.at[0, w], partner) for w in range(n_w)]
    own_z = [
        [rcopy(w_refs[w], wz.at[d, w], zs.at[d, w], zr.at[d, w], stride[d]) for d in order]
        for w in range(n_w)
    ]
    forwards = [
        [rcopy(wz.at[d, w], wx.at[d + 1, w], ps.at[d + 1, w], pr.at[d + 1, w], partner) for d in order]
        for w in range(n_w)
    ]

    def send_z(w):
        for d in order:
            own_z[w][d].start()

    for w in range(3):
        send_z(w)
        own_x[w].start()
    for w in range(3, n_w):
        send_z(w)
    for c in x_copies:
        c.wait_recv()
    per = width_x // block
    depth = width_x * nt
    chunks = [(t, x_ref)] + [((t + nt - 1 - d) % nt, xbuf.at[d]) for d in range(nt - 1)]
    mean = sum(jnp.sum(r[...].astype(F32), axis=1, keepdims=True) for _, r in chunks) / depth
    var = (
        sum(jnp.sum(jnp.square(r[...].astype(F32) - mean), axis=1, keepdims=True) for _, r in chunks)
        / depth
    )
    inv = lax.rsqrt(var + 1e-05)
    for src, r in chunks:
        y = (r[...].astype(F32) - mean) * inv
        for p in range(per):
            b = src * per + p
            g = gain_ref[:, pl.ds(pl.multiple_of(b * block, block), block)]
            normed[b] = (y[:, p * block : (p + 1) * block] * g).astype(BF16)
    pre = dot(normed[0], wg_ref[0:block, :])
    for b in range(1, n):
        pre = pre + dot(normed[b], wg_ref[b * block : (b + 1) * block, :])

    def relay(w):
        for d in order:
            own_z[w][d].wait_recv()
            forwards[w][d].start()

    def near_half(w):
        value = dot(normed[s], w_refs[w][...])
        for d in order:
            value = value + dot(normed[came(d, x)], wz[d, w])
        acc[w] = value

    def far_half(w):
        own_x[w].wait_recv()
        value = acc[w] + dot(normed[z * 2 + (1 - x)], wx[0, w])
        for d in order:
            forwards[w][d].wait_recv()
            value = value + dot(normed[came(d, 1 - x)], wx[d + 1, w])
        acc[w] = value

    for w in range(3):
        relay(w)
        near_half(w)
    own_x[3].start()
    own_x[4].start()
    for w in range(3):
        far_half(w)

    span = rows
    pre_rows = jnp.transpose(pre)
    which = lax.broadcasted_iota(jnp.int32, (8, span), 0)
    shift_lane = lax.broadcasted_iota(jnp.int32, shift_ref.shape, 1)
    shift_rows = jnp.zeros((8, span), F32)
    pace_rows = jnp.zeros((8, span), F32)
    jolt_rows = jnp.zeros((8, span), F32)
    for h in range(heads):
        mine = jnp.sum(
            jnp.where(shift_lane == t * heads + h, shift_ref[...], 0.0), axis=1, keepdims=True
        )
        for e in range(2):
            here = which == e * heads + h
            shift_rows = jnp.where(here, mine[e : e + 1, :], shift_rows)
            pace_rows = jnp.where(here, pace_ref[e, h : h + 1, :], pace_rows)
            jolt_rows = jnp.where(here, jolt_ref[e, h : h + 1, :], jolt_rows)
    beta = jax.nn.sigmoid(pre_rows[0:8] + shift_rows)
    log_decay = -pace_rows * jax.nn.softplus(pre_rows[8:16]) + jolt_rows
    i = lax.broadcasted_iota(jnp.int32, (span, span), 0)
    j = lax.broadcasted_iota(jnp.int32, (span, span), 1)
    high = lax.Precision.HIGHEST
    upto = jnp.dot(log_decay, (i <= j).astype(F32), precision=high, preferred_element_type=F32)
    onto = jnp.dot(log_decay, (i >= j).astype(F32), precision=high, preferred_element_type=F32)
    cum = jnp.where(which < heads, upto, onto)
    cols = jnp.transpose(jnp.concatenate([beta, cum, jnp.zeros((112, span), F32)], axis=0))
    eye = (i == j).astype(F32)
    eye_head = (
        lax.broadcasted_iota(jnp.int32, (HEAD, HEAD), 0)
        == lax.broadcasted_iota(jnp.int32, (HEAD, HEAD), 1)
    ).astype(F32)
    level = i ^ j
    within = []
    for h in range(heads):
        lo = h * HEAD
        q = jax.nn.silu(acc[0, :, lo : lo + HEAD].astype(BF16).astype(F32))
        k = jax.nn.silu(acc[1, :, lo : lo + HEAD].astype(BF16).astype(F32))
        k = k * lax.rsqrt(jnp.sum(jnp.square(k), axis=1, keepdims=True) + 1e-06)
        v = acc[2, :, lo : lo + HEAD].astype(BF16).astype(F32)
        kt = jnp.transpose(k)
        kk = dot3(k, kt)
        qk = dot(q.astype(BF16), kt.astype(BF16))
        total = jnp.zeros((span, HEAD), F32)
        for e in range(2):
            c = e * heads + h
            beta_col = cols[:, c : c + 1]
            cum_col = cols[:, 8 + c : 9 + c]
            cum_row = cum[c : c + 1, :]
            keep = (i >= j) if e == 0 else (i <= j)
            gap = jnp.exp(jnp.where(keep, cum_col - cum_row, 0.0))
            decay = jnp.where(keep, gap, 0.0)
            below = jnp.where(i == j, 0.0, beta_col * kk * decay)
            inverse = eye - jnp.where(level < 2, below, 0.0)
            size = 2
            while size < span:
                corner = jnp.where((level >= size) & (level < 2 * size), below, 0.0)
                low = inverse.astype(BF16)
                reach = dot(corner.astype(BF16), low)
                inverse = inverse - dot(low, reach.astype(BF16))
                size = 2 * size
            residual = (eye - inverse) - dot3(below, inverse)
            inverse = inverse + dot(inverse.astype(BF16), residual.astype(BF16))
            grown = jnp.exp(cum_col)
            rhs = jnp.concatenate([v * beta_col, k * (beta_col * grown)], axis=1)
            solved = dot3(inverse, rhs)
            solved_b = solved.astype(BF16)
            out = dot((qk * decay).astype(BF16), solved_b)
            total = total + out[:, :HEAD]
            reads[c] = (q * grown - out[:, HEAD:]).astype(BF16)
            end = cum[c : c + 1, span - 1 : span] if e == 0 else cum[c : c + 1, 0:1]
            tail = jnp.transpose(k * jnp.exp(end - cum_col))
            state = dot3(tail, solved)
            maps[c, :, :HEAD] = (jnp.exp(end) * eye_head - state[:, HEAD:]).astype(BF16)
            maps[c, :, HEAD:] = state[:, :HEAD].astype(BF16)
            if h == 0:
                relay(3 + e)
        within.append(total)

    edge = 16

    def at(offset):
        return ((s + offset + n) % n, t)

    def inside(offset):
        return (s < n - offset) if offset > 0 else (s >= -offset)

    def start(moves):
        for go, copy, _ in moves:
            @pl.when(inside(go))
            def _():
                copy.start()

    def arrive(moves):
        for go, copy, slot in moves:
            @pl.when(inside(-go))
            def _():
                copy.wait_recv()

            @pl.when(jnp.logical_not(inside(-go)))
            def _():
                slot[...] = jnp.zeros(slot.shape, slot.dtype)

    def left(moves):
        for go, copy, _ in moves:
            @pl.when(inside(go))
            def _():
                copy.wait_send()

    steps = []
    for d in (1, 2):
        for e in range(2):
            go = d if e == 0 else -d
            slot = near.at[e, d - 1]
            steps.append((go, rcopy(maps.at[pl.ds(e * heads, heads)], slot, ns.at[e, d - 1], nr.at[e, d - 1], at(go)), slot))
    start(steps)
    own_x[n_in].start()
    relay(n_in)

    for w in range(3, n_in):
        near_half(w)
    for w in range(3, n_in):
        far_half(w)
    glu_value = acc[3].astype(BF16).astype(F32)
    glu_gate = acc[4].astype(BF16).astype(F32)
    gated = (glu_value * jax.nn.sigmoid(glu_gate)).astype(BF16)
    edges[0] = gated[0:edge]
    edges[1] = gated[rows - edge : rows]
    sides = [
        (1, rcopy(edges.at[1], halo.at[0], hs.at[0], hr.at[0], at(1)), halo.at[0]),
        (-1, rcopy(edges.at[0], halo.at[1], hs.at[1], hr.at[1], at(-1)), halo.at[1]),
    ]
    start(sides)
    arrive(steps)
    for e in range(2):
        for h in range(heads):
            first = near[e, 0, h]
            mixed = dot(first[:, :HEAD], near[e, 1, h])
            pair[e, h, :, :HEAD] = mixed[:, :HEAD].astype(BF16)
            pair[e, h, :, HEAD:] = (mixed[:, HEAD:] + first[:, HEAD:].astype(F32)).astype(BF16)
    hops = []
    for d in range(1, half):
        for e in range(2):
            go = 2 * d if e == 0 else -2 * d
            slot = far.at[e, d - 1]
            hops.append((go, rcopy(pair.at[e], slot, fs.at[e, d - 1], fr.at[e, d - 1], at(go)), slot))
    start(hops)
    for w in range(n_in + 1, n_w):
        own_x[w].start()

    conv_pad[edge : edge + rows, :] = gated.astype(F32)
    arrive(sides)
    conv_pad[0:edge, :] = halo[0].astype(F32)
    conv_pad[edge + rows : 2 * edge + rows, :] = halo[1].astype(F32)
    taps = taps_ref[...].astype(F32)
    count = taps.shape[0]
    base = edge - count // 2
    filtered = conv_pad[base : base + rows, :] * taps[0:1, :]
    for tap in range(1, count):
        filtered = filtered + conv_pad[base + tap : base + tap + rows, :] * taps[tap : tap + 1, :]
    sum_col = jnp.sum(filtered, axis=1, keepdims=True)
    square_col = jnp.sum(filtered * filtered, axis=1, keepdims=True)
    lane = lax.broadcasted_iota(jnp.int32, (rows, 128), 1)
    stat[...] = jnp.transpose(jnp.where(lane == 0, sum_col, jnp.where(lane == 1, square_col, 0.0)))[0:8]
    stat_copies = [rcopy(stat, stats.at[d], ss.at[d], sr.at[d], others[d]) for d in range(nt - 1)]
    for c in stat_copies:
        c.start()
    for w in range(n_in + 1, n_w):
        relay(w)
    for c in stat_copies:
        c.wait_recv()
    whole = stat[...]
    for d in range(nt - 1):
        whole = whole + stats[d]
    back = jnp.transpose(jnp.concatenate([whole, jnp.zeros((120, rows), F32)], axis=0))
    mean = back[:, 0:1] / channels
    second = back[:, 1:2] / channels
    conv_out = jax.nn.silu(
        (filtered - mean) * lax.rsqrt(second - mean * mean + 1e-05) * cgain_ref[...]
    ).astype(BF16)

    arrive(hops)
    delta_heads = []
    for h in range(heads):
        o = within[h]
        for e in range(2):
            entry = jnp.zeros((HEAD, HEAD), F32)
            for d in range(half - 2, -1, -1):
                m = far[e, d, h]
                entry = dot(m[:, :HEAD], entry.astype(BF16)) + m[:, HEAD:].astype(F32)
            m = pair[e, h]
            entry = dot(m[:, :HEAD], entry.astype(BF16)) + m[:, HEAD:].astype(F32)
            o = o + dot(reads[e * heads + h], entry.astype(BF16))
        o = o * lax.rsqrt(jnp.mean(jnp.square(o), axis=1, keepdims=True) + 1e-06) * hgain_ref[...]
        delta_heads.append(o.astype(BF16))
    delta_out = jnp.concatenate(delta_heads, axis=1)
    piece = rows // nt
    sums = []

    def emit(first, second):
        at_block = len(sums)
        value = (dot(delta_out, first) + dot(conv_out, second)).astype(BF16)
        for p in range(nt):
            part[at_block, p] = value[p * piece : (p + 1) * piece]
        copies = [
            rcopy(part.at[at_block, (t + d) % nt], parts.at[d - 1, at_block], rs.at[d - 1, at_block], rr.at[d - 1, at_block], others[d - 1])
            for d in range(1, nt)
        ]
        for c in copies:
            c.start()
        sums.append(copies)

    sources = [s]
    emit(w_refs[n_in][...], w_refs[n_in + 1][...])
    for d in order:
        sources.append(came(d, x))
        emit(wz[d, n_in], wz[d, n_in + 1])
    sources.append(z * 2 + (1 - x))
    own_x[n_in].wait_recv()
    own_x[n_in + 1].wait_recv()
    emit(wx[0, n_in], wx[0, n_in + 1])
    for d in order:
        forwards[n_in][d].wait_recv()
        forwards[n_in + 1][d].wait_recv()
        sources.append(came(d, 1 - x))
        emit(wx[d + 1, n_in], wx[d + 1, n_in + 1])
    out_block = w_refs[n_in].shape[1]
    for b in range(n):
        mixed = part[b, t].astype(F32)
        for d in range(nt - 1):
            sums[b][d].wait_recv()
            mixed = mixed + parts[d, b].astype(F32)
        out_ref[:, pl.ds(pl.multiple_of(sources[b] * out_block, out_block), out_block)] = mixed.astype(BF16)
    left(steps)
    left(sides)
    left(hops)
    for group in own_z + forwards + sums + [x_copies, own_x, stat_copies]:
        for c in group:
            c.wait_send()


def fast_device(
    n, nt,
    inputs, in_gain, query_weight, key_weight, value_weight, beta_weight, decay_weight,
    beta_shift, decay_pace, decay_jolt, head_gain, glu_value_weight, glu_gate_weight,
    conv_kernel, conv_gain, out_delta_weight, out_conv_weight,
):
    rows, width_x = inputs.shape
    block, width = query_weight.shape
    heads = decay_pace.shape[1]
    half = n // 2
    depth = in_gain.shape[0]
    channels = conv_kernel.shape[1] * nt
    first = lax.axis_index("tp") * heads

    def gate_columns(weight):
        own = lax.dynamic_slice_in_dim(weight, first, heads, 2)
        own = jnp.moveaxis(own, 0, 1).reshape(depth, 2 * heads)
        return jnp.pad(own, ((0, 0), (0, 8 - 2 * heads)))

    gate_weight = jnp.pad(
        jnp.concatenate([gate_columns(beta_weight), gate_columns(decay_weight)], axis=1),
        ((0, 0), (0, 112)),
    )
    weights = (
        query_weight, key_weight, value_weight, glu_value_weight, glu_gate_weight,
        out_delta_weight, out_conv_weight,
    )
    n_w = len(weights)
    out_block = out_delta_weight.shape[1]
    piece = rows // nt
    dma = pltpu.SemaphoreType.DMA
    return pl.pallas_call(
        functools.partial(layer_kernel, n, nt, heads, channels),
        name="layer",
        out_shape=jax.ShapeDtypeStruct((piece, out_block * n), BF16),
        in_specs=[VM] * (9 + n_w),
        out_specs=VM,
        scratch_shapes=[
            pltpu.VMEM((nt - 1, rows, width_x), BF16),
            pltpu.VMEM((n, rows, block), BF16),
            pltpu.VMEM((n_w - 2, rows, width), F32),
            pltpu.VMEM((half - 1, n_w, block, width), BF16),
            pltpu.VMEM((half, n_w, block, width), BF16),
            pltpu.VMEM((2 * heads, HEAD, 2 * HEAD), BF16),
            pltpu.VMEM((2 * heads, rows, HEAD), BF16),
            pltpu.VMEM((2, 2, heads, HEAD, 2 * HEAD), BF16),
            pltpu.VMEM((2, heads, HEAD, 2 * HEAD), BF16),
            pltpu.VMEM((2, half - 1, heads, HEAD, 2 * HEAD), BF16),
            pltpu.VMEM((2, 16, width), BF16),
            pltpu.VMEM((2, 16, width), BF16),
            pltpu.VMEM((rows + 32, width), F32),
            pltpu.VMEM((8, rows), F32),
            pltpu.VMEM((nt - 1, 8, rows), F32),
            pltpu.VMEM((n, nt, piece, out_block), BF16),
            pltpu.VMEM((nt - 1, n, piece, out_block), BF16),
            dma((nt - 1,)), dma((nt - 1,)),
            dma((half - 1, n_w)), dma((half - 1, n_w)),
            dma((half, n_w)), dma((half, n_w)),
            dma((2, 2)), dma((2, 2)),
            dma((2, half - 1)), dma((2, half - 1)),
            dma((2,)), dma((2,)),
            dma((nt - 1,)), dma((nt - 1,)),
            dma((nt - 1, n)), dma((nt - 1, n)),
        ],
        compiler_params=pltpu.CompilerParams(collective_id=0, has_side_effects=True),
    )(
        inputs, in_gain.reshape(1, depth), gate_weight, beta_shift, decay_pace, decay_jolt,
        conv_kernel, conv_gain.reshape(1, width), head_gain.reshape(1, HEAD), *weights,
    )


def device_program(n, nt, *args):
    inputs, query_weight, pace = args[0], args[2], args[8]
    heads = pace.shape[1]
    block, width = query_weight.shape
    suits = (
        n % 2 == 0 and n >= 4 and nt >= 2
        and block % 128 == 0 and width % 128 == 0 and width == heads * HEAD
        and 2 * heads <= 8 and inputs.shape[1] % block == 0 and args[15].shape[1] % 128 == 0
        and args[13].shape[1] == width and args[15].shape == (block, width) and V_HEADS == QK_HEADS
        and inputs.shape[0] & (inputs.shape[0] - 1) == 0
        and inputs.shape[0] % 128 == 0 and (inputs.shape[0] // nt) % 16 == 0
        and inputs.shape[0] <= 256 and KERNEL <= 33 and n <= 16
    )
    return fast_device(n, nt, *args) if suits else on_device(*args)


def solution(mesh):
    return jax.shard_map(
        functools.partial(device_program, mesh.shape["sp"], mesh.shape["tp"]),
        mesh=mesh,
        in_specs=(
            P("sp", "tp"),
            P(),
            P("sp", "tp"),
            P("sp", "tp"),
            P("sp", "tp"),
            P(),
            P(),
            P(),
            P(None, "tp", "sp"),
            P(None, "tp", "sp"),
            P(),
            P("sp", "tp"),
            P("sp", "tp"),
            P(None, "tp"),
            P("tp"),
            P("tp", "sp"),
            P("tp", "sp"),
        ),
        out_specs=P(("sp", "tp"), None),
        check_vma=False,
    )
```
